32 devices in a mesh: ep: 8 (over z, y), tp: 4 (over x, core).
Axes of the slice: x: 2, y: 2, z: 4, core: 2. Of those that a mesh axis runs over, the one named last changes fastest.
Arguments:
- mixer_in: bfloat16 [4096, 4096], P(('ep', 'tp')), may hold values from -6 to 6
- mixer_gain: float32 [4096], replicated, may hold values from 0.1 to 1.9
- group_weight: bfloat16 [4, 1024, 1024], P('tp'), may hold values from -0.1875 to 0.1875
- group_scale: float32 [4, 1024], P('tp'), may hold values from 0.1 to 1.9
- expert_in: bfloat16 [4096, 4096], P(('ep', 'tp')), may hold values from -6 to 6
- expert_gain: float32 [4096], replicated, may hold values from 0.1 to 1.9
- routes: int32 [4096, 2], P('ep'), may hold values from 0 to 7, all different within a row; in each aligned block of 128 rows (0 to 127, 128 to 255, ...) at most 48 rows name the same one
- route_weight: float32 [4096, 2], P('ep'), may hold values from 0.2 to 1
- gate_weight: bfloat16 [8, 4096, 1024], P('ep', None, 'tp'), may hold values from -0.25 to 0.25
- up_weight: bfloat16 [8, 4096, 1024], P('ep', None, 'tp'), may hold values from -0.25 to 0.25
- down_weight: bfloat16 [8, 1024, 4096], P('ep', 'tp'), may hold values from -0.02734375 to 0.02734375
Outputs:
- mixed: bfloat16 [4096, 4096], P('ep', 'tp')
- expert_out: bfloat16 [4096, 4096], P(('ep', 'tp'))
The draws below stay inside these ranges and needn't reach their ends.
Inputs may be any that keep to these rules, and one draw needn't show every extreme that they name: `routes`: each row names 2 different experts; within the rows of one device (aligned blocks of 128 rows) no expert is named more than 48 times, and that count is reached.
All inputs are finite; a program needn't handle non-finite values.
Results may differ from the reference program's by a relative error of at most 0.012.
Values may be sent and summed in bfloat16 or wider, within the bound.
A program may use at most 128 MiB of HBM per device.

```python
import math
import jax
import jax.numpy as jnp
import numpy as np
from jax import lax

D = 4096
GROUPS = 4
GW = 1024
WMAX = 16
F = 1024
TOP = 2
TOK_B = 128
EXPERTS = 8
CAP = 48
TOKENS_A = 4096
TOKENS_B = 4096
N_TP = 4


def levels(rng, dims, cuts, low, high):
    loudness, own = 1.0, jax.random.fold_in(rng, 6)
    for axis_at, blocks in cuts:
        steps = jnp.exp(jax.random.uniform(jax.random.fold_in(own, axis_at), (blocks,), jnp.float32, low / len(cuts), high / len(cuts)))
        loudness = loudness * jnp.repeat(steps, dims[axis_at] // blocks).reshape([-1 if axis == axis_at else 1 for axis in range(len(dims))])
    return loudness


def assign_block(rng, own, number, rows, amount, top, bound, slope):
    ranking = jax.random.permutation(rng, amount)
    packed, ordinary = portions_of(amount, rows * top, bound, slope, True), portions_of(amount, rows * top, bound, slope, False)
    places = jnp.arange(amount)

    def named(tallies, offset_by):
        used = int((tallies > 0).sum())
        fixed = max(1, used // 4)
        shifted = fixed + (places - fixed + offset_by * (used - fixed)) % max(1, amount - fixed)
        return jnp.zeros((amount,), jnp.int32).at[ranking[jnp.where(places < fixed, places, shifted)]].set(jnp.asarray(tallies, jnp.int32))

    tallies = jnp.where(number % 4 == 0, named(packed, number // 4), named(ordinary, number - number // 4 - 1))
    mixed = jax.random.permutation(jax.random.fold_in(own, 3), amount)
    source_of, receiver = mixed[0:amount // 2 * 2:2], mixed[1:amount // 2 * 2:2]
    slack = jnp.minimum(tallies[source_of] - 1, bound - tallies[receiver]) // 2
    slack = jnp.where((source_of == ranking[0]) | (receiver == ranking[0]) | (tallies[receiver] == 0), 0, jnp.maximum(slack, 0))
    shifted = jax.random.randint(jax.random.fold_in(own, 4), (amount // 2,), 0, 1 << 20) % (slack + 1)
    tallies = tallies.at[source_of].add(-shifted).at[receiver].add(shifted)
    members = jnp.searchsorted(jnp.cumsum(tallies), jnp.arange(rows * top), side="right").astype(jnp.int32)
    listing = members.reshape(top, rows).T
    listing = listing[jax.random.permutation(jax.random.fold_in(own, 1), rows)]
    offset_by = jax.random.randint(jax.random.fold_in(own, 2), (rows, 1), 0, top)
    return jnp.take_along_axis(listing, (jnp.arange(top)[None, :] + offset_by) % top, axis=1)


def portions_of(amount, total, bound, skew, full):
    portions = [(1 << 20) // math.isqrt(rank ** skew) + 1 for rank in range(1, amount + 1)]
    largest = bound if full else min(bound, max(-(-total // amount), total * portions[0] // sum(portions)))
    least = 1 if total - largest >= amount - 1 else 0
    given, surplus = [largest] + [least] * (amount - 1), total - largest - least * (amount - 1)
    while surplus > 0:
        movable = [i for i in range(1, amount) if given[i] < largest] or [i for i in range(1, amount) if given[i] < bound]
        mass, budget = sum([portions[i] for i in movable]), surplus
        for i in movable:
            more = min(bound - given[i], max(1, budget * portions[i] // mass), surplus)
            given[i] = given[i] + more
            surplus = surplus - more
    return np.array(given)


def bell_draw(own_key, extent, width, bound, cuts=(), kind=jnp.bfloat16):
    result = width * jax.random.normal(own_key, extent, jnp.float32)
    if cuts:
        result = result * levels(own_key, extent, cuts, -0.22, 0.18)
    return jnp.clip(result, -bound, bound).astype(kind)


def setup_inputs(seed: int = 0) -> dict:
    key_of = jax.random.split(jax.random.key(seed), 12)
    mixer_in = bell_draw(key_of[0], (TOKENS_A, D), 1.0, 6.0, ((0, 32),))
    mixer_gain = jnp.clip(1.0 + 0.18 * jax.random.normal(key_of[1], (D,), jnp.float32), 0.1, 1.9)
    group_weight = bell_draw(key_of[2], (GROUPS, GW, GW), GW ** -0.5, 0.1875, ((0, 4),))
    group_scale = jnp.clip(1.0 + 0.18 * jax.random.normal(key_of[3], (GROUPS, GW), jnp.float32), 0.1, 1.9)
    expert_in = bell_draw(key_of[4], (TOKENS_B, D), 1.0, 6.0, ((0, 32),))
    expert_gain = jnp.clip(1.0 + 0.18 * jax.random.normal(key_of[5], (D,), jnp.float32), 0.1, 1.9)
    routes_keys = jax.random.split(jax.random.fold_in(key_of[6], 1), TOKENS_B // TOK_B)
    routes_turns = jax.random.permutation(jax.random.fold_in(key_of[6], 3), TOKENS_B // TOK_B)
    routes = jax.vmap(lambda own, number: assign_block(jax.random.fold_in(key_of[6], 2), own, number, TOK_B, EXPERTS, TOP, CAP, 2))(routes_keys, routes_turns).reshape((TOKENS_B, TOP))
    route_weight = jnp.clip(0.2 + 0.8 * jax.random.uniform(key_of[7], (TOKENS_B, TOP), jnp.float32) ** levels(key_of[7], (TOKENS_B, TOP), ((0, 8),), -0.2, 0.2), 0.2, 1.0)
    gate_weight = bell_draw(key_of[8], (EXPERTS, D, F), (D // 9) ** -0.5, 0.25, ((0, 8), (2, 4)))
    up_weight = bell_draw(key_of[9], (EXPERTS, D, F), (D // 9) ** -0.5, 0.25, ((0, 8), (2, 4)))
    down_weight = bell_draw(key_of[10], (EXPERTS, F, D), (45 * F) ** -0.5, 0.02734375, ((0, 8), (1, 4)))
    return {"mixer_in": mixer_in, "mixer_gain": mixer_gain, "group_weight": group_weight, "group_scale": group_scale, "expert_in": expert_in, "expert_gain": expert_gain, "routes": routes, "route_weight": route_weight, "gate_weight": gate_weight, "up_weight": up_weight, "down_weight": down_weight}


epsilon = 1e-06
clamp_limit = 7.0
sigmoid_slope = 1.702

def rms_norm(values, gain):
    widened = values.astype(jnp.float32)
    scaled = widened * lax.rsqrt(lax.optimization_barrier(jnp.mean(widened * widened, axis=-1, keepdims=True)) + epsilon)
    return (scaled * gain).astype(jnp.bfloat16)

def clamped_unit(gate_part, up_part):
    gate_part = jnp.minimum(gate_part, clamp_limit)
    up_part = jnp.clip(up_part, -clamp_limit, clamp_limit)
    return ((up_part + 1.0) * gate_part * jax.nn.sigmoid(sigmoid_slope * gate_part)).astype(jnp.bfloat16)

def slot_table(block_routes, experts, capacity):
    count = block_routes.shape[0]
    onehot = (block_routes[:, :, None] == jnp.arange(experts, dtype=jnp.int32)[None, None, :]).astype(jnp.int32)
    per_token = lax.optimization_barrier(jnp.sum(onehot, axis=1))
    earlier = jnp.cumsum(per_token, axis=0) - per_token
    slot_rank = lax.optimization_barrier(jnp.sum(onehot * earlier[:, None, :], axis=2))
    matches = onehot[:, :, :, None] * (slot_rank[:, :, None, None] == jnp.arange(capacity, dtype=jnp.int32)[None, None, None, :]).astype(jnp.int32)
    source = lax.optimization_barrier(jnp.sum(matches * jnp.arange(count, dtype=jnp.int32)[:, None, None, None], axis=(0, 1)))
    filled = lax.optimization_barrier(jnp.sum(matches, axis=(0, 1)))
    return (source, filled, slot_rank)

def reference(mixer_in, mixer_gain, group_weight, group_scale, expert_in, expert_gain, routes, route_weight, gate_weight, up_weight, down_weight):
    normed = rms_norm(mixer_in, mixer_gain)
    length = normed.shape[0]
    position = jnp.arange(length, dtype=jnp.int32)
    pieces = []
    for group in range(GROUPS):
        window = 2 ** (group + 1)
        values = normed[:, group * GW:(group + 1) * GW].astype(jnp.float32)
        padded = jnp.pad(values, ((WMAX - 1, 0), (0, 0)))
        window_sum = jnp.zeros_like(values)
        for offset in range(window):
            window_sum = window_sum + padded[WMAX - 1 - offset:WMAX - 1 - offset + length]
        counts = jnp.minimum(position + 1, window).astype(jnp.float32)[:, None]
        pooled = (window_sum / counts - values).astype(jnp.bfloat16)
        product = jnp.dot(pooled, group_weight[group], preferred_element_type=jnp.float32)
        pieces.append((product * group_scale[group]).astype(jnp.bfloat16))
    mixed = jnp.concatenate(pieces, axis=1)
    expert_norm = rms_norm(expert_in, expert_gain)
    blocks = expert_norm.shape[0] // TOK_B
    block_routes = routes.reshape(blocks, TOK_B, TOP)
    source, filled, slot_rank = lax.map(lambda item: slot_table(item, EXPERTS, CAP), block_routes)
    global_index = source + (jnp.arange(blocks, dtype=jnp.int32) * TOK_B)[:, None, None]
    part_width = F // N_TP

    def one_expert(expert):
        slot_index = lax.dynamic_index_in_dim(global_index, expert, 1, keepdims=False).reshape(-1)
        present = lax.dynamic_index_in_dim(filled, expert, 1, keepdims=False).reshape(-1)
        picked = expert_norm[slot_index] * present[:, None].astype(jnp.bfloat16)
        gate_part = jnp.dot(picked, gate_weight[expert], preferred_element_type=jnp.float32)
        up_part = jnp.dot(picked, up_weight[expert], preferred_element_type=jnp.float32)
        hidden = clamped_unit(gate_part, up_part)
        total = jnp.zeros((picked.shape[0], picked.shape[1]), jnp.float32)
        for part in range(N_TP):
            partial_value = jnp.dot(hidden[:, part * part_width:(part + 1) * part_width], down_weight[expert][part * part_width:(part + 1) * part_width], preferred_element_type=jnp.float32).astype(jnp.bfloat16)
            total = total + lax.optimization_barrier(partial_value).astype(jnp.float32)
        return total.astype(jnp.bfloat16).reshape(blocks, CAP, picked.shape[1])
    results = lax.map(one_expert, jnp.arange(EXPERTS, dtype=jnp.int32))
    flat_rows = results.reshape(-1, results.shape[-1])
    block_of = (jnp.arange(expert_norm.shape[0], dtype=jnp.int32) // TOK_B)[:, None]
    slot_index = (routes * blocks + block_of) * CAP + slot_rank.reshape(-1, TOP)
    expert_sum = jnp.zeros(expert_norm.shape, jnp.float32)
    for choice_slot in range(TOP):
        expert_sum = expert_sum + flat_rows[slot_index[:, choice_slot]].astype(jnp.float32) * route_weight[:, choice_slot:choice_slot + 1]
    return (mixed, expert_sum.astype(jnp.bfloat16))
```

```python
import functools
import jax
import jax.numpy as jnp
from jax import lax
from jax.experimental import pallas as pl
from jax.experimental.pallas import tpu as pltpu
from jax.sharding import PartitionSpec as P

WMAX = 16
NORM_ROWS = 16
K_CHUNKS = 8
D_CHUNKS = 8

epsilon = 1e-06
clamp_limit = 7.0
sigmoid_slope = 1.702

MESH = pl.DeviceIdType.MESH


def clamped_unit(gate_part, up_part):
    gate_part = jnp.minimum(gate_part, clamp_limit)
    up_part = jnp.clip(up_part, -clamp_limit, clamp_limit)
    return ((up_part + 1.0) * gate_part * jax.nn.sigmoid(sigmoid_slope * gate_part)).astype(
        jnp.bfloat16
    )


def norm_rows(source, gain, at):
    widened = source[pl.ds(at, NORM_ROWS), :].astype(jnp.float32)
    mean = jnp.sum(widened * widened, axis=-1, keepdims=True) * (1.0 / widened.shape[-1])
    return (widened * lax.rsqrt(mean + epsilon) * gain[...]).astype(jnp.bfloat16)


def aligned(value, size):
    return pl.multiple_of(value * size, size)


def kernel(
    n_ep,
    n_tp,
    mixer_in,
    mixer_gain,
    group_weight,
    group_scale,
    expert_in,
    expert_gain,
    routes,
    route_weight,
    gate_w,
    up_w,
    down_w,
    mixed_out,
    expert_out,
    x_in,
    m_in,
    e_gain,
    m_gain,
    scale,
    named,
    shares,
    gate_b,
    up_b,
    down_b,
    normed,
    pick,
    share_high,
    share_low,
    outgoing,
    arrived,
    acc_gate,
    acc_up,
    hidden,
    result,
    returned,
    m_normed,
    m_rows,
    g_weight,
    m_out,
    e_out,
    load_sem,
    gate_send,
    gate_recv,
    up_send,
    up_recv,
    down_send,
    down_recv,
    out_send,
    out_recv,
    ret_send,
    ret_recv,
    mix_send,
    mix_recv,
    halo_send,
    halo_recv,
    m_store,
    e_store,
):
    ep = lax.axis_index("ep")
    tp = lax.axis_index("tp")
    tokens, width = x_in.shape
    group_width = g_weight.shape[0]
    slots, units = hidden.shape
    capacity = arrived.shape[1]
    part_units = units // n_tp
    k_size = width // K_CHUNKS
    d_size = width // D_CHUNKS

    def peer(i):
        return lax.rem(ep + i, n_ep)

    loads = [
        pltpu.make_async_copy(source, target, load_sem.at[i])
        for i, (source, target) in enumerate(
            [
                (expert_in, x_in),
                (expert_gain, e_gain),
                (routes, named),
                (route_weight, shares),
                (mixer_in, m_in),
                (mixer_gain, m_gain),
                (group_scale, scale),
                (group_weight.at[0], g_weight),
            ]
        )
    ]
    for load in loads:
        load.start()

    barrier = pltpu.get_barrier_semaphore()
    for r in range(1, n_tp):
        pl.semaphore_signal(barrier, inc=1, device_id={"tp": tp ^ r}, device_id_type=MESH)

    @pl.loop(1, n_ep)
    def _(i):
        pl.semaphore_signal(barrier, inc=1, device_id={"ep": peer(i)}, device_id_type=MESH)

    def weight_copy(kind, r, j):
        low = r & -r
        if kind == "down":
            source, target, send, recv = down_w, down_b, down_send, down_recv
            span = (slice(None), pl.ds(aligned(j, d_size), d_size))
        else:
            source, target = (gate_w, gate_b) if kind == "gate" else (up_w, up_b)
            send, recv = (gate_send, gate_recv) if kind == "gate" else (up_send, up_recv)
            span = (pl.ds(aligned(j, k_size), k_size), slice(None))
        origin = source.at[(0,) + span] if r == low else target.at[(r ^ low,) + span]
        if r == 0:
            return pltpu.make_async_copy(origin, target.at[(0,) + span], recv.at[0, j])
        return pltpu.make_async_remote_copy(
            src_ref=origin,
            dst_ref=target.at[(r,) + span],
            send_sem=send.at[r, j],
            recv_sem=recv.at[r, j],
            device_id={"tp": tp ^ low},
            device_id_type=MESH,
        )

    bits = []
    while (1 << len(bits)) < n_tp:
        bits.insert(0, 1 << len(bits))
    own_targets = bits
    forwards = {r: [r | b for b in bits if b < (r & -r)] for r in range(1, n_tp)}
    order = [0] + sorted(range(1, n_tp), key=lambda r: (r & (n_tp // 2) > 0, bin(r).count("1")))

    @pl.loop(0, K_CHUNKS)
    def _(j):
        weight_copy("gate", 0, j).start()
        weight_copy("up", 0, j).start()

    pl.semaphore_wait(barrier, n_ep - 1 + n_tp - 1)

    for target in own_targets:

        @pl.loop(0, K_CHUNKS)
        def _(j):
            weight_copy("gate", target, j).start()
            weight_copy("up", target, j).start()

    for load in loads[:4]:
        load.wait()
    mine = pl.ds(aligned(tp, tokens), tokens)
    own = named[:, mine]
    own_share = shares[:, mine]
    top = own.shape[0]
    experts = lax.broadcasted_iota(jnp.int32, (n_ep, tokens), 0)
    onehot = [
        (experts == jnp.broadcast_to(own[k : k + 1, :], (n_ep, tokens))).astype(jnp.float32)
        for k in range(top)
    ]
    per_token = functools.reduce(lambda a, b: a + b, onehot)
    before = (
        lax.broadcasted_iota(jnp.int32, (tokens, tokens), 0)
        < lax.broadcasted_iota(jnp.int32, (tokens, tokens), 1)
    ).astype(jnp.bfloat16)
    earlier = jnp.dot(per_token.astype(jnp.bfloat16), before, preferred_element_type=jnp.float32)
    slot_rows = lax.broadcasted_iota(jnp.int32, (slots, tokens), 0)
    picked = jnp.zeros((slots, tokens), jnp.float32)
    spread = jnp.zeros((slots, tokens), jnp.float32)
    for k in range(top):
        rank = jnp.sum(onehot[k] * earlier, axis=0, keepdims=True).astype(jnp.int32)
        slot = own[k : k + 1, :] * capacity + rank
        match = slot_rows == jnp.broadcast_to(slot, (slots, tokens))
        picked = picked + jnp.where(match, 1.0, 0.0)
        spread = spread + jnp.where(
            match, jnp.broadcast_to(own_share[k : k + 1, :], (slots, tokens)), 0.0
        )
    pick[...] = picked.reshape(n_ep, capacity, tokens).astype(jnp.bfloat16)
    spread = spread.T
    high = spread.astype(jnp.bfloat16)
    share_high[...] = high
    share_low[...] = (spread - high.astype(jnp.float32)).astype(jnp.bfloat16)

    @pl.loop(0, tokens // NORM_ROWS)
    def _(i):
        at = aligned(i, NORM_ROWS)
        normed[pl.ds(at, NORM_ROWS), :] = norm_rows(x_in, e_gain, at)

    def send_rows(i):
        return pltpu.make_async_remote_copy(
            src_ref=outgoing.at[peer(i)],
            dst_ref=arrived.at[ep],
            send_sem=out_send.at[i],
            recv_sem=out_recv.at[i],
            device_id={"ep": peer(i)},
            device_id_type=MESH,
        )

    @pl.loop(1, n_ep)
    def _(i):
        outgoing[peer(i)] = jnp.dot(
            pick[peer(i)], normed[...], preferred_element_type=jnp.float32
        ).astype(jnp.bfloat16)
        send_rows(i).start()

    arrived[ep] = jnp.dot(pick[ep], normed[...], preferred_element_type=jnp.float32).astype(
        jnp.bfloat16
    )

    @pl.loop(0, D_CHUNKS)
    def _(j):
        weight_copy("down", 0, j).start()

    for target in own_targets:

        @pl.loop(0, D_CHUNKS)
        def _(j):
            weight_copy("down", target, j).start()

    for load in loads[4:]:
        load.wait()

    @pl.loop(0, tokens // NORM_ROWS)
    def _(i):
        at = aligned(i, NORM_ROWS)
        rows = norm_rows(m_in, m_gain, at)
        for g in range(n_tp):
            m_normed[g, pl.ds(at, NORM_ROWS), :] = rows[:, g * group_width : (g + 1) * group_width]

    own_rows = pl.ds(pl.multiple_of(WMAX + tp * tokens, WMAX), tokens)

    def send_mix(r):
        return pltpu.make_async_remote_copy(
            src_ref=m_normed.at[tp ^ r],
            dst_ref=m_rows.at[own_rows, :],
            send_sem=mix_send.at[r],
            recv_sem=mix_recv.at[r],
            device_id={"tp": tp ^ r},
            device_id_type=MESH,
        )

    for r in range(1, n_tp):
        send_mix(r).start()
    m_rows[own_rows, :] = m_normed[tp]

    half = n_tp // 2
    early = K_CHUNKS - 2

    def forward(kind, r, j):
        if forwards[r]:
            weight_copy(kind, r, j).wait_recv()
            for target in forwards[r]:
                weight_copy(kind, target, j).start()

    def forward_all(kinds, j):
        for r in order[1:]:
            for kind in kinds:
                forward(kind, r, j)

    def arrive(kinds, r, j):
        if r == 0:
            for kind in kinds:
                weight_copy(kind, 0, j).wait()
        elif not forwards[r]:
            for kind in kinds:
                weight_copy(kind, r, j).wait_recv()

    def accumulate(r, j, first):
        rows = arrived[:, :, pl.ds(aligned(j, k_size), k_size)].reshape(slots, k_size)
        span = pl.ds(aligned(j, k_size), k_size)
        for acc, weight in ((acc_gate, gate_b), (acc_up, up_b)):
            product = jnp.dot(rows, weight[r, span, :], preferred_element_type=jnp.float32)
            if first:
                acc[r] = product
            else:
                acc[r] += product

    both = ("gate", "up")

    @pl.loop(0, early)
    def _(j):
        forward_all(both, j)

    @pl.loop(1, n_ep)
    def _(i):
        pltpu.make_async_remote_copy(
            src_ref=outgoing.at[peer(i)],
            dst_ref=arrived.at[lax.rem(ep + n_ep - i, n_ep)],
            send_sem=out_send.at[i],
            recv_sem=out_recv.at[i],
            device_id={"ep": peer(i)},
            device_id_type=MESH,
        ).wait_recv()

    def chunk(j, first, forwarding):
        if forwarding:
            forward_all(both, j)
        for r in order:
            arrive(both, r, j)
            accumulate(r, j, first)

    chunk(0, True, False)

    @pl.loop(1, early)
    def _(j):
        chunk(j, False, False)

    @pl.loop(early, K_CHUNKS)
    def _(j):
        chunk(j, False, True)

    for r in range(n_tp):
        hidden[:, r * part_units : (r + 1) * part_units] = clamped_unit(acc_gate[r], acc_up[r])

    def send_back(j, i):
        return pltpu.make_async_remote_copy(
            src_ref=result.at[j, peer(i)],
            dst_ref=returned.at[j, ep],
            send_sem=ret_send.at[j, i],
            recv_sem=ret_recv.at[j, i],
            device_id={"ep": peer(i)},
            device_id_type=MESH,
        )

    @pl.loop(0, D_CHUNKS)
    def _(j):
        forward_all(("down",), j)
        for r in order:
            arrive(("down",), r, j)
        weight = down_b[:, :, pl.ds(aligned(j, d_size), d_size)].reshape(units, d_size)
        product = jnp.dot(hidden[...], weight, preferred_element_type=jnp.float32)
        result[j] = product.astype(jnp.bfloat16).reshape(n_ep, capacity, d_size)

        @pl.loop(1, n_ep)
        def _(i):
            send_back(j, i).start()

        returned[j, ep] = result[j, ep]

    for r in range(1, n_tp):
        theirs = pl.ds(pl.multiple_of(WMAX + (tp ^ r) * tokens, WMAX), tokens)
        pltpu.make_async_remote_copy(
            src_ref=m_normed.at[tp ^ r],
            dst_ref=m_rows.at[theirs, :],
            send_sem=mix_send.at[r],
            recv_sem=mix_recv.at[r],
            device_id={"tp": tp ^ r},
            device_id_type=MESH,
        ).wait_recv()
    halo = pltpu.make_async_remote_copy(
        src_ref=m_rows.at[n_tp * tokens : n_tp * tokens + WMAX, :],
        dst_ref=m_rows.at[0:WMAX, :],
        send_sem=halo_send,
        recv_sem=halo_recv,
        device_id={"ep": peer(1)},
        device_id_type=MESH,
    )
    halo.start()
    halo.wait_recv()
    window = 2 << tp
    span_rows = tokens + WMAX
    here = lax.broadcasted_iota(jnp.int32, (tokens, span_rows), 0)
    there = lax.broadcasted_iota(jnp.int32, (tokens, span_rows), 1)
    back = here + WMAX - there
    inside = (back >= 0) & (back < window)
    row = lax.broadcasted_iota(jnp.int32, (tokens, 1), 0)
    stores = []
    for b in range(n_tp):
        position = (ep * n_tp + b) * tokens
        band = (inside & (there + position >= WMAX)).astype(jnp.bfloat16)
        values = m_rows[b * tokens : b * tokens + span_rows, :]
        total = jnp.dot(band, values, preferred_element_type=jnp.float32)
        counts = jnp.minimum(row + position + 1, window).astype(jnp.float32)
        pooled = (total / counts - values[WMAX:, :].astype(jnp.float32)).astype(jnp.bfloat16)
        product = jnp.dot(pooled, g_weight[...], preferred_element_type=jnp.float32)
        m_out[b] = (product * scale[...]).astype(jnp.bfloat16)
        store = pltpu.make_async_copy(
            m_out.at[b], mixed_out.at[b * tokens : (b + 1) * tokens, :], m_store.at[b]
        )
        store.start()
        stores.append(store)

    def write_out(j):
        return pltpu.make_async_copy(
            e_out.at[j], expert_out.at[:, pl.ds(aligned(j, d_size), d_size)], e_store.at[j]
        )

    @pl.loop(0, D_CHUNKS)
    def _(j):
        @pl.loop(1, n_ep)
        def _(i):
            pltpu.make_async_remote_copy(
                src_ref=result.at[j, peer(i)],
                dst_ref=returned.at[j, lax.rem(ep + n_ep - i, n_ep)],
                send_sem=ret_send.at[j, i],
                recv_sem=ret_recv.at[j, i],
                device_id={"ep": peer(i)},
                device_id_type=MESH,
            ).wait_recv()

        rows = returned[j].reshape(slots, d_size)
        e_out[j] = (
            jnp.dot(share_high[...], rows, preferred_element_type=jnp.float32)
            + jnp.dot(share_low[...], rows, preferred_element_type=jnp.float32)
        ).astype(jnp.bfloat16)
        write_out(j).start()

    for r in range(1, n_tp):

        @pl.loop(0, K_CHUNKS)
        def _(j):
            weight_copy("gate", r, j).wait_send()
            weight_copy("up", r, j).wait_send()

        @pl.loop(0, D_CHUNKS)
        def _(j):
            weight_copy("down", r, j).wait_send()

        send_mix(r).wait_send()
    halo.wait_send()

    @pl.loop(1, n_ep)
    def _(i):
        send_rows(i).wait_send()

    @pl.loop(0, D_CHUNKS)
    def _(j):
        @pl.loop(1, n_ep)
        def _(i):
            send_back(j, i).wait_send()

        write_out(j).wait()

    for store in stores:
        store.wait()


def shards(
    mixer_in,
    mixer_gain,
    group_weight,
    group_scale,
    expert_in,
    expert_gain,
    routes,
    route_weight,
    gate_weight,
    up_weight,
    down_weight,
):
    n_ep = lax.axis_size("ep")
    n_tp = lax.axis_size("tp")
    tokens, width = expert_in.shape
    group_width = group_weight.shape[-1]
    block_tokens, top = routes.shape
    part_units = gate_weight.shape[-1]
    units = part_units * n_tp
    capacity = max(2, 3 * tokens * top // (2 * n_ep))
    capacity = -(-capacity // 8) * 8
    slots = n_ep * capacity
    d_size = width // D_CHUNKS
    bf16, f32 = jnp.bfloat16, jnp.float32
    vmem = pltpu.VMEM
    dma = pltpu.SemaphoreType.DMA
    anywhere = pl.BlockSpec(memory_space=pl.ANY)
    scratch = [
        vmem((tokens, width), bf16),
        vmem((tokens, width), bf16),
        vmem((1, width), f32),
        vmem((1, width), f32),
        vmem((1, group_width), f32),
        vmem((top, block_tokens), jnp.int32),
        vmem((top, block_tokens), f32),
        vmem((n_tp, width, part_units), bf16),
        vmem((n_tp, width, part_units), bf16),
        vmem((n_tp, part_units, width), bf16),
        vmem((tokens, width), bf16),
        vmem((n_ep, capacity, tokens), bf16),
        vmem((tokens, slots), bf16),
        vmem((tokens, slots), bf16),
        vmem((n_ep, capacity, width), bf16),
        vmem((n_ep, capacity, width), bf16),
        vmem((n_tp, slots, part_units), f32),
        vmem((n_tp, slots, part_units), f32),
        vmem((slots, units), bf16),
        vmem((D_CHUNKS, n_ep, capacity, d_size), bf16),
        vmem((D_CHUNKS, n_ep, capacity, d_size), bf16),
        vmem((n_tp, tokens, group_width), bf16),
        vmem((WMAX + n_tp * tokens, group_width), bf16),
        vmem((group_width, group_width), bf16),
        vmem((n_tp, tokens, group_width), bf16),
        vmem((D_CHUNKS, tokens, d_size), bf16),
        dma((8,)),
        dma((n_tp, K_CHUNKS)),
        dma((n_tp, K_CHUNKS)),
        dma((n_tp, K_CHUNKS)),
        dma((n_tp, K_CHUNKS)),
        dma((n_tp, D_CHUNKS)),
        dma((n_tp, D_CHUNKS)),
        dma((n_ep,)),
        dma((n_ep,)),
        dma((D_CHUNKS, n_ep)),
        dma((D_CHUNKS, n_ep)),
        dma((n_tp,)),
        dma((n_tp,)),
        dma(()),
        dma(()),
        dma((n_tp,)),
        dma((D_CHUNKS,)),
    ]
    flops = 6 * slots * width * units + 2 * n_tp * tokens * group_width * group_width
    return pl.pallas_call(
        functools.partial(kernel, n_ep, n_tp),
        out_shape=(
            jax.ShapeDtypeStruct((n_tp * tokens, group_width), bf16),
            jax.ShapeDtypeStruct((tokens, width), bf16),
        ),
        in_specs=[anywhere] * 11,
        out_specs=(anywhere, anywhere),
        scratch_shapes=scratch,
        compiler_params=pltpu.CompilerParams(
            collective_id=0, has_side_effects=True, vmem_limit_bytes=67043328
        ),
        cost_estimate=pl.CostEstimate(flops=flops, bytes_accessed=1 << 26, transcendentals=0),
    )(
        mixer_in,
        mixer_gain.reshape(1, width),
        group_weight,
        group_scale,
        expert_in,
        expert_gain.reshape(1, width),
        routes.T,
        route_weight.T,
        gate_weight,
        up_weight,
        down_weight,
    )


def solution(mesh):
    in_specs = (
        P(("ep", "tp"), None),
        P(),
        P("tp", None, None),
        P("tp", None),
        P(("ep", "tp"), None),
        P(),
        P("ep", None),
        P("ep", None),
        P("ep", None, "tp"),
        P("ep", None, "tp"),
        P("ep", "tp", None),
    )
    out_specs = (P("ep", "tp"), P(("ep", "tp"), None))
    return jax.shard_map(shards, mesh=mesh, in_specs=in_specs, out_specs=out_specs, check_vma=False)
```

```python
import functools
import jax
import jax.numpy as jnp
from jax import lax
from jax.experimental import pallas as pl
from jax.experimental.pallas import tpu as pltpu
from jax.sharding import PartitionSpec as P

WMAX = 16
NORM_ROWS = 16
K_CHUNKS = 8
D_CHUNKS = 8

epsilon = 1e-06
clamp_limit = 7.0
sigmoid_slope = 1.702

MESH = pl.DeviceIdType.MESH


def clamped_unit(gate_part, up_part):
    gate_part = jnp.minimum(gate_part, clamp_limit)
    up_part = jnp.clip(up_part, -clamp_limit, clamp_limit)
    return ((up_part + 1.0) * gate_part * jax.nn.sigmoid(sigmoid_slope * gate_part)).astype(
        jnp.bfloat16
    )


def norm_rows(source, gain, at):
    widened = source[pl.ds(at, NORM_ROWS), :].astype(jnp.float32)
    mean = jnp.sum(widened * widened, axis=-1, keepdims=True) * (1.0 / widened.shape[-1])
    return (widened * lax.rsqrt(mean + epsilon) * gain[...]).astype(jnp.bfloat16)


def aligned(value, size):
    return pl.multiple_of(value * size, size)


def kernel(
    n_ep,
    n_tp,
    mixer_in,
    mixer_gain,
    group_weight,
    group_scale,
    expert_in,
    expert_gain,
    routes,
    route_weight,
    gate_w,
    up_w,
    down_w,
    mixed_out,
    expert_out,
    x_in,
    m_in,
    e_gain,
    m_gain,
    scale,
    named,
    shares,
    gate_up,
    down_b,
    normed,
    pick,
    share_high,
    share_low,
    outgoing,
    arrived,
    acc,
    hidden_out,
    hidden,
    result,
    returned,
    m_normed,
    m_rows,
    m_tail,
    g_weight,
    m_out,
    e_out,
    load_sem,
    down_send,
    down_recv,
    out_send,
    out_recv,
    row_send,
    row_recv,
    hid_send,
    hid_recv,
    ret_send,
    ret_recv,
    mix_send,
    mix_recv,
    tail_send,
    tail_recv,
    halo_send,
    halo_recv,
    m_store,
    e_store,
):
    ep = lax.axis_index("ep")
    tp = lax.axis_index("tp")
    tokens, width = x_in.shape
    group_width = g_weight.shape[0]
    n_groups, group, sub, units = hidden.shape
    rounds = n_groups // 2
    slots = n_ep * rounds * sub
    part_units = units // n_tp
    k_size = width // K_CHUNKS
    d_size = width // D_CHUNKS

    def peer(i):
        return jnp.bitwise_xor(ep, i)

    loads = [
        pltpu.make_async_copy(origin, target, load_sem.at[i])
        for i, (origin, target) in enumerate(
            [
                (expert_in, x_in),
                (expert_gain, e_gain),
                (routes, named),
                (route_weight, shares),
                (gate_w.at[0], gate_up.at[:, 0:part_units]),
                (up_w.at[0], gate_up.at[:, part_units : 2 * part_units]),
                (mixer_in, m_in),
                (mixer_gain, m_gain),
                (group_scale, scale),
                (group_weight.at[0], g_weight),
            ]
        )
    ]
    for load in loads:
        load.start()

    barrier = pltpu.get_barrier_semaphore()
    for r in range(1, n_tp):
        pl.semaphore_signal(barrier, inc=1, device_id={"tp": tp ^ r}, device_id_type=MESH)

    @pl.loop(1, n_ep)
    def _(i):
        pl.semaphore_signal(barrier, inc=1, device_id={"ep": peer(i)}, device_id_type=MESH)

    bits = []
    while (1 << len(bits)) < n_tp:
        bits.insert(0, 1 << len(bits))
    forwards = {r: [r | b for b in bits if r == 0 or b < (r & -r)] for r in range(n_tp)}
    order = [0] + sorted(range(1, n_tp), key=lambda r: (r & (n_tp // 2) > 0, bin(r).count("1")))
    relays = [r for r in order[1:] if forwards[r]]
    leaves = [r for r in order[1:] if not forwards[r]]

    def down_copy(r, j):
        low = r & -r
        span = (slice(None), pl.ds(aligned(j, d_size), d_size))
        origin = down_w.at[(0,) + span] if r == low else down_b.at[(r ^ low,) + span]
        if r == 0:
            return pltpu.make_async_copy(origin, down_b.at[(0,) + span], down_recv.at[0, j])
        return pltpu.make_async_remote_copy(
            src_ref=origin,
            dst_ref=down_b.at[(r,) + span],
            send_sem=down_send.at[r, j],
            recv_sem=down_recv.at[r, j],
            device_id={"tp": tp ^ low},
            device_id_type=MESH,
        )

    def row_copy(r, u, i):
        low = r & -r
        return pltpu.make_async_remote_copy(
            src_ref=arrived.at[u, i, r ^ low],
            dst_ref=arrived.at[u, i, r],
            send_sem=row_send.at[r, u, i],
            recv_sem=row_recv.at[r, u, i],
            device_id={"tp": tp ^ low},
            device_id_type=MESH,
        )

    def start_down(first, last):
        @pl.loop(first, last)
        def _(j):
            for r in forwards[0]:
                down_copy(r, j).start()

    @pl.loop(0, D_CHUNKS)
    def _(j):
        down_copy(0, j).start()

    pl.semaphore_wait(barrier, n_ep - 1 + n_tp - 1)
    start_down(0, 1)

    for load in loads[:4]:
        load.wait()
    mine = pl.ds(aligned(tp, tokens), tokens)
    own = named[:, mine]
    own_share = shares[:, mine]
    top = own.shape[0]
    experts = lax.broadcasted_iota(jnp.int32, (n_ep, tokens), 0)
    onehot = [
        (experts == jnp.broadcast_to(own[k : k + 1, :], (n_ep, tokens))).astype(jnp.float32)
        for k in range(top)
    ]
    per_token = functools.reduce(lambda a, b: a + b, onehot)
    before = (
        lax.broadcasted_iota(jnp.int32, (tokens, tokens), 0)
        < lax.broadcasted_iota(jnp.int32, (tokens, tokens), 1)
    ).astype(jnp.bfloat16)
    earlier = jnp.dot(per_token.astype(jnp.bfloat16), before, preferred_element_type=jnp.float32)
    slot_rows = lax.broadcasted_iota(jnp.int32, (slots, tokens), 0)
    picked = jnp.zeros((slots, tokens), jnp.float32)
    spread = jnp.zeros((slots, tokens), jnp.float32)
    shift = sub.bit_length() - 1
    for k in range(top):
        rank = jnp.sum(onehot[k] * earlier, axis=0, keepdims=True).astype(jnp.int32)
        away = jnp.bitwise_xor(own[k : k + 1, :], ep)
        turn = lax.shift_right_logical(rank, jnp.full_like(rank, shift))
        far = jnp.where(away >= group, 1, 0)
        slot = ((far * rounds + turn) * group + away - far * group) * sub + rank - turn * sub
        match = slot_rows == jnp.broadcast_to(slot, (slots, tokens))
        picked = picked + jnp.where(match, 1.0, 0.0)
        spread = spread + jnp.where(
            match, jnp.broadcast_to(own_share[k : k + 1, :], (slots, tokens)), 0.0
        )
    picked = picked.reshape(2, rounds, group * sub, tokens).astype(jnp.bfloat16)
    for half in range(2):
        pick[:, half * group * sub : (half + 1) * group * sub, :] = picked[half]
    spread = spread.T
    high = spread.astype(jnp.bfloat16)
    share_high[...] = high
    share_low[...] = (spread - high.astype(jnp.float32)).astype(jnp.bfloat16)

    @pl.loop(0, tokens // NORM_ROWS)
    def _(i):
        at = aligned(i, NORM_ROWS)
        normed[pl.ds(at, NORM_ROWS), :] = norm_rows(x_in, e_gain, at)

    def send_rows(u, i):
        half = u // rounds
        return pltpu.make_async_remote_copy(
            src_ref=outgoing.at[u, i],
            dst_ref=arrived.at[u, i, 0],
            send_sem=out_send.at[u, i],
            recv_sem=out_recv.at[u, i],
            device_id={"ep": peer(half * group + i)},
            device_id_type=MESH,
        )

    sequence = [0, rounds] + list(range(1, rounds)) + list(range(rounds + 1, n_groups))

    def send_group(u):
        @pl.loop(0 if u >= rounds else 1, group)
        def _(i):
            send_rows(u, i).start()

    for k in range(rounds):
        rows = jnp.dot(pick[k], normed[...], preferred_element_type=jnp.float32)
        rows = rows.astype(jnp.bfloat16).reshape(2, group, sub, width)
        arrived[k, 0, 0] = rows[0, 0]
        for half in range(2):
            outgoing[half * rounds + k] = rows[half]
        for r in forwards[0]:
            row_copy(r, k, 0).start()
        for u in (0, rounds) if k == 0 else (k,):
            send_group(u)
    for u in range(rounds + 1, n_groups):
        send_group(u)

    for load in loads[4:]:
        load.wait()

    @pl.loop(0, tokens // NORM_ROWS)
    def _(i):
        at = aligned(i, NORM_ROWS)
        rows = norm_rows(m_in, m_gain, at)
        for g in range(n_tp):
            m_normed[g, pl.ds(at, NORM_ROWS), :] = rows[:, g * group_width : (g + 1) * group_width]

    own_rows = pl.ds(pl.multiple_of(WMAX + tp * tokens, WMAX), tokens)
    m_rows[own_rows, :] = m_normed[tp]

    last = n_tp - 1

    def tail_copy(r):
        return pltpu.make_async_remote_copy(
            src_ref=m_normed.at[last ^ r, tokens - WMAX : tokens, :],
            dst_ref=m_tail,
            send_sem=tail_send.at[r],
            recv_sem=tail_recv,
            device_id={"tp": tp ^ r},
            device_id_type=MESH,
        )

    halo = pltpu.make_async_remote_copy(
        src_ref=m_tail,
        dst_ref=m_rows.at[0:WMAX, :],
        send_sem=halo_send,
        recv_sem=halo_recv,
        device_id={"ep": lax.rem(ep + 1, n_ep)},
        device_id_type=MESH,
    )

    @pl.when(tp == last)
    def _():
        for r in range(1, n_tp):
            tail_copy(r).start()
        m_tail[...] = m_normed[last, tokens - WMAX : tokens, :]


    def send_mix(r):
        return pltpu.make_async_remote_copy(
            src_ref=m_normed.at[tp ^ r],
            dst_ref=m_rows.at[own_rows, :],
            send_sem=mix_send.at[r],
            recv_sem=mix_recv.at[r],
            device_id={"tp": tp ^ r},
            device_id_type=MESH,
        )

    def take(u):
        @pl.loop(0 if u >= rounds else 1, group)
        def _(i):
            send_rows(u, i).wait_recv()
            for r in forwards[0]:
                row_copy(r, u, i).start()

    def relay(u):
        for r in relays:

            @pl.loop(0, group)
            def _(i):
                row_copy(r, u, i).wait_recv()
                for target in forwards[r]:
                    row_copy(target, u, i).start()

    def hid_copy(r, u):
        return pltpu.make_async_remote_copy(
            src_ref=hidden_out.at[u, r],
            dst_ref=hidden.at[u, :, :, r * part_units : (r + 1) * part_units],
            send_sem=hid_send.at[r, u],
            recv_sem=hid_recv.at[r, u],
            device_id={"tp": tp ^ r},
            device_id_type=MESH,
        )

    def work(u):
        for r in leaves:

            @pl.loop(0, group)
            def _(i):
                row_copy(r, u, i).wait_recv()

        @pl.loop(0, K_CHUNKS)
        def _(k):
            span = pl.ds(aligned(k, k_size), k_size)
            rows = arrived[u, :, :, :, span].reshape(group * n_tp * sub, k_size)
            product = jnp.dot(rows, gate_up[span, :], preferred_element_type=jnp.float32)

            @pl.when(k == 0)
            def _():
                acc[...] = product

            @pl.when(k > 0)
            def _():
                acc[...] += product

        units_of = clamped_unit(acc[:, :part_units], acc[:, part_units:])
        units_of = units_of.reshape(group, n_tp, sub, part_units)
        hidden[u, :, :, 0:part_units] = units_of[:, 0]
        for r in range(1, n_tp):
            hidden_out[u, r] = units_of[:, r]
            hid_copy(r, u).start()

    for step in range(len(sequence) + 2):
        if step < len(sequence):
            take(sequence[step])
        if step == min(1, len(sequence) - 1):

            @pl.when(tp != last)
            def _():
                tail_copy(1).wait_recv()

            halo.start()
        if step == len(sequence) and step >= 2:
            work(sequence[step - 2])
        if 1 <= step <= len(sequence):
            relay(sequence[step - 1])
        if step >= 2 and step != len(sequence) or step == len(sequence) + 1:
            work(sequence[step - 2])

    start_down(1, D_CHUNKS)
    for r in range(1, n_tp):
        send_mix(r).start()

    for u in sequence:
        for r in range(1, n_tp):
            hid_copy(r, u).wait_recv()

    def send_back(j, half, i):
        block = (j, slice(half * rounds, (half + 1) * rounds), i)
        return pltpu.make_async_remote_copy(
            src_ref=result.at[block],
            dst_ref=returned.at[block],
            send_sem=ret_send.at[j, half, i],
            recv_sem=ret_recv.at[j, half, i],
            device_id={"ep": peer(half * group + i)},
            device_id_type=MESH,
        )

    def down_arrive(j):
        down_copy(0, j).wait()
        for r in relays:
            down_copy(r, j).wait_recv()
            for target in forwards[r]:
                down_copy(target, j).start()
        for r in leaves:
            down_copy(r, j).wait_recv()

    @pl.loop(0, D_CHUNKS)
    def _(j):
        down_arrive(j)
        weight = down_b[:, :, pl.ds(aligned(j, d_size), d_size)].reshape(units, d_size)
        rows = hidden[...].reshape(slots, units)
        product = jnp.dot(rows, weight, preferred_element_type=jnp.float32)
        result[j] = product.astype(jnp.bfloat16).reshape(n_groups, group, sub, d_size)

        for half in (1, 0):

            @pl.loop(1 - half, group)
            def _(i):
                send_back(j, half, i).start()

        returned[j, 0:rounds, 0] = result[j, 0:rounds, 0]

    for r in range(1, n_tp):
        theirs = pl.ds(pl.multiple_of(WMAX + (tp ^ r) * tokens, WMAX), tokens)
        pltpu.make_async_remote_copy(
            src_ref=m_normed.at[tp ^ r],
            dst_ref=m_rows.at[theirs, :],
            send_sem=mix_send.at[r],
            recv_sem=mix_recv.at[r],
            device_id={"tp": tp ^ r},
            device_id_type=MESH,
        ).wait_recv()
    halo.wait_recv()
    window = 2 << tp
    span_rows = tokens + WMAX
    here = lax.broadcasted_iota(jnp.int32, (tokens, span_rows), 0)
    there = lax.broadcasted_iota(jnp.int32, (tokens, span_rows), 1)
    back = here + WMAX - there
    inside = (back >= 0) & (back < window)
    row = lax.broadcasted_iota(jnp.int32, (tokens, 1), 0)
    stores = []
    for b in range(n_tp):
        position = (ep * n_tp + b) * tokens
        band = (inside & (there + position >= WMAX)).astype(jnp.bfloat16)
        values = m_rows[b * tokens : b * tokens + span_rows, :]
        total = jnp.dot(band, values, preferred_element_type=jnp.float32)
        counts = jnp.minimum(row + position + 1, window).astype(jnp.float32)
        pooled = (total / counts - values[WMAX:, :].astype(jnp.float32)).astype(jnp.bfloat16)
        product = jnp.dot(pooled, g_weight[...], preferred_element_type=jnp.float32)
        m_out[b] = (product * scale[...]).astype(jnp.bfloat16)
        store = pltpu.make_async_copy(
            m_out.at[b], mixed_out.at[b * tokens : (b + 1) * tokens, :], m_store.at[b]
        )
        store.start()
        stores.append(store)

    def write_out(j):
        return pltpu.make_async_copy(
            e_out.at[j], expert_out.at[:, pl.ds(aligned(j, d_size), d_size)], e_store.at[j]
        )

    @pl.loop(0, D_CHUNKS)
    def _(j):
        for half in range(2):

            @pl.loop(1 - half, group)
            def _(i):
                send_back(j, half, i).wait_recv()

        rows = returned[j].reshape(slots, d_size)
        e_out[j] = (
            jnp.dot(share_high[...], rows, preferred_element_type=jnp.float32)
            + jnp.dot(share_low[...], rows, preferred_element_type=jnp.float32)
        ).astype(jnp.bfloat16)
        write_out(j).start()

    for r in range(1, n_tp):

        @pl.loop(0, D_CHUNKS)
        def _(j):
            down_copy(r, j).wait_send()

        @pl.loop(0, n_groups)
        def _(u):
            hid_copy(r, u).wait_send()

        @pl.loop(0, n_groups)
        def _(u):
            @pl.loop(0, group)
            def _(i):
                row_copy(r, u, i).wait_send()

        send_mix(r).wait_send()
    halo.wait_send()

    @pl.when(tp == last)
    def _():
        for r in range(1, n_tp):
            tail_copy(r).wait_send()

    for half in range(2):

        @pl.loop(1 - half, group)
        def _(i):
            for u in range(half * rounds, (half + 1) * rounds):
                send_rows(u, i).wait_send()

            @pl.loop(0, D_CHUNKS)
            def _(j):
                send_back(j, half, i).wait_send()

    @pl.loop(0, D_CHUNKS)
    def _(j):
        write_out(j).wait()

    for store in stores:
        store.wait()


def shards(
    mixer_in,
    mixer_gain,
    group_weight,
    group_scale,
    expert_in,
    expert_gain,
    routes,
    route_weight,
    gate_weight,
    up_weight,
    down_weight,
):
    n_ep = lax.axis_size("ep")
    n_tp = lax.axis_size("tp")
    tokens, width = expert_in.shape
    group_width = group_weight.shape[-1]
    block_tokens, top = routes.shape
    part_units = gate_weight.shape[-1]
    units = part_units * n_tp
    capacity = max(2, 3 * tokens * top // (2 * n_ep))
    capacity = -(-capacity // 8) * 8
    slots = n_ep * capacity
    sub = 16 if capacity % 16 == 0 else 8
    rounds = capacity // sub
    groups = 2 * rounds
    group = n_ep // 2
    d_size = width // D_CHUNKS
    bf16, f32 = jnp.bfloat16, jnp.float32
    vmem = pltpu.VMEM
    dma = pltpu.SemaphoreType.DMA
    anywhere = pl.BlockSpec(memory_space=pl.ANY)
    scratch = [
        vmem((tokens, width), bf16),
        vmem((tokens, width), bf16),
        vmem((1, width), f32),
        vmem((1, width), f32),
        vmem((1, group_width), f32),
        vmem((top, block_tokens), jnp.int32),
        vmem((top, block_tokens), f32),
        vmem((width, 2 * part_units), bf16),
        vmem((n_tp, part_units, width), bf16),
        vmem((tokens, width), bf16),
        vmem((rounds, n_ep * sub, tokens), bf16),
        vmem((tokens, slots), bf16),
        vmem((tokens, slots), bf16),
        vmem((groups, group, sub, width), bf16),
        vmem((groups, group, n_tp, sub, width), bf16),
        vmem((group * n_tp * sub, 2 * part_units), f32),
        vmem((groups, n_tp, group, sub, part_units), bf16),
        vmem((groups, group, sub, units), bf16),
        vmem((D_CHUNKS, groups, group, sub, d_size), bf16),
        vmem((D_CHUNKS, groups, group, sub, d_size), bf16),
        vmem((n_tp, tokens, group_width), bf16),
        vmem((WMAX + n_tp * tokens, group_width), bf16),
        vmem((WMAX, group_width), bf16),
        vmem((group_width, group_width), bf16),
        vmem((n_tp, tokens, group_width), bf16),
        vmem((D_CHUNKS, tokens, d_size), bf16),
        dma((10,)),
        dma((n_tp, D_CHUNKS)),
        dma((n_tp, D_CHUNKS)),
        dma((groups, group)),
        dma((groups, group)),
        dma((n_tp, groups, group)),
        dma((n_tp, groups, group)),
        dma((n_tp, groups)),
        dma((n_tp, groups)),
        dma((D_CHUNKS, 2, group)),
        dma((D_CHUNKS, 2, group)),
        dma((n_tp,)),
        dma((n_tp,)),
        dma((n_tp,)),
        dma(()),
        dma(()),
        dma(()),
        dma((n_tp,)),
        dma((D_CHUNKS,)),
    ]
    flops = 6 * slots * width * units + 2 * n_tp * tokens * group_width * group_width
    return pl.pallas_call(
        functools.partial(kernel, n_ep, n_tp),
        out_shape=(
            jax.ShapeDtypeStruct((n_tp * tokens, group_width), bf16),
            jax.ShapeDtypeStruct((tokens, width), bf16),
        ),
        in_specs=[anywhere] * 11,
        out_specs=(anywhere, anywhere),
        scratch_shapes=scratch,
        compiler_params=pltpu.CompilerParams(
            collective_id=0, has_side_effects=True, vmem_limit_bytes=67043328
        ),
        cost_estimate=pl.CostEstimate(flops=flops, bytes_accessed=1 << 26, transcendentals=0),
    )(
        mixer_in,
        mixer_gain.reshape(1, width),
        group_weight,
        group_scale,
        expert_in,
        expert_gain.reshape(1, width),
        routes.T,
        route_weight.T,
        gate_weight,
        up_weight,
        down_weight,
    )


def solution(mesh):
    in_specs = (
        P(("ep", "tp"), None),
        P(),
        P("tp", None, None),
        P("tp", None),
        P(("ep", "tp"), None),
        P(),
        P("ep", None),
        P("ep", None),
        P("ep", None, "tp"),
        P("ep", None, "tp"),
        P("ep", "tp", None),
    )
    out_specs = (P("ep", "tp"), P(("ep", "tp"), None))
    return jax.shard_map(shards, mesh=mesh, in_specs=in_specs, out_specs=out_specs, check_vma=False)
```

```python
import functools
import jax
import jax.numpy as jnp
from jax import lax
from jax.experimental import pallas as pl
from jax.experimental.pallas import tpu as pltpu
from jax.sharding import PartitionSpec as P

WMAX = 16
NORM_ROWS = 16
K_CHUNKS = 8
D_CHUNKS = 8
FIRST = 1
SECOND = 2

epsilon = 1e-06
clamp_limit = 7.0
sigmoid_slope = 1.702

MESH = pl.DeviceIdType.MESH


def clamped_unit(gate_part, up_part):
    gate_part = jnp.minimum(gate_part, clamp_limit)
    up_part = jnp.clip(up_part, -clamp_limit, clamp_limit)
    return ((up_part + 1.0) * gate_part * jax.nn.sigmoid(sigmoid_slope * gate_part)).astype(
        jnp.bfloat16
    )


def norm_rows(source, gain, at):
    widened = source[pl.ds(at, NORM_ROWS), :].astype(jnp.float32)
    mean = jnp.sum(widened * widened, axis=-1, keepdims=True) * (1.0 / widened.shape[-1])
    return (widened * lax.rsqrt(mean + epsilon) * gain[...]).astype(jnp.bfloat16)


def aligned(value, size):
    return pl.multiple_of(value * size, size)


def kernel(
    n_ep,
    n_tp,
    mixer_in,
    mixer_gain,
    group_weight,
    group_scale,
    expert_in,
    expert_gain,
    routes,
    route_weight,
    gate_w,
    up_w,
    down_w,
    mixed_out,
    expert_out,
    x_in,
    m_in,
    e_gain,
    m_gain,
    scale,
    named,
    shares,
    gate_up,
    down_b,
    normed,
    pick,
    share_near,
    share_far,
    share_in,
    outgoing,
    arrived,
    acc,
    hidden_out,
    hidden,
    result,
    returned,
    gathered,
    partial_out,
    partial_in,
    m_normed,
    m_rows,
    m_tail,
    g_weight,
    m_out,
    e_out,
    load_sem,
    down_send,
    down_recv,
    out_send,
    out_recv,
    row_send,
    row_recv,
    hid_send,
    hid_recv,
    ret_send,
    ret_recv,
    share_send,
    share_recv,
    col_send,
    col_recv,
    part_send,
    part_recv,
    mix_send,
    mix_recv,
    tail_send,
    tail_recv,
    halo_send,
    halo_recv,
    m_store,
    e_store,
):
    ep = lax.axis_index("ep")
    tp = lax.axis_index("tp")
    tokens, width = x_in.shape
    group_width = g_weight.shape[0]
    n_groups, group, sub, units = hidden.shape
    rounds = n_groups // 2
    slots = n_ep * rounds * sub
    quarter = n_ep // 4
    lag = 1
    near_lag = 2
    part_units = units // n_tp
    k_size = width // K_CHUNKS
    d_size = width // D_CHUNKS

    def peer(i):
        return jnp.bitwise_xor(ep, i)

    inner = jnp.bitwise_xor(lax.rem(lax.div(ep, quarter), 2), lax.div(ep, group))

    loads = [
        pltpu.make_async_copy(origin, target, load_sem.at[i])
        for i, (origin, target) in enumerate(
            [
                (expert_in, x_in),
                (expert_gain, e_gain),
                (routes, named),
                (route_weight, shares),
                (gate_w.at[0], gate_up.at[:, 0:part_units]),
                (up_w.at[0], gate_up.at[:, part_units : 2 * part_units]),
                (mixer_in, m_in),
                (mixer_gain, m_gain),
                (group_scale, scale),
                (group_weight.at[0], g_weight),
            ]
        )
    ]
    for load in loads:
        load.start()

    barrier = pltpu.get_barrier_semaphore()
    for r in range(1, n_tp):
        pl.semaphore_signal(barrier, inc=1, device_id={"tp": tp ^ r}, device_id_type=MESH)

    @pl.loop(1, n_ep)
    def _(i):
        pl.semaphore_signal(barrier, inc=1, device_id={"ep": peer(i)}, device_id_type=MESH)

    bits = []
    while (1 << len(bits)) < n_tp:
        bits.insert(0, 1 << len(bits))
    forwards = {r: [r | b for b in bits if r == 0 or b < (r & -r)] for r in range(n_tp)}
    order = [0] + sorted(range(1, n_tp), key=lambda r: (r & (n_tp // 2) > 0, bin(r).count("1")))
    relays = [r for r in order[1:] if forwards[r]]
    leaves = [r for r in order[1:] if not forwards[r]]

    def down_copy(r, j):
        low = r & -r
        span = (slice(None), pl.ds(aligned(j, d_size), d_size))
        origin = down_w.at[(0,) + span] if r == low else down_b.at[(r ^ low,) + span]
        if r == 0:
            return pltpu.make_async_copy(origin, down_b.at[(0,) + span], down_recv.at[0, j])
        return pltpu.make_async_remote_copy(
            src_ref=origin,
            dst_ref=down_b.at[(r,) + span],
            send_sem=down_send.at[r, j],
            recv_sem=down_recv.at[r, j],
            device_id={"tp": tp ^ low},
            device_id_type=MESH,
        )

    def row_copy(r, u, i):
        low = r & -r
        return pltpu.make_async_remote_copy(
            src_ref=arrived.at[u, i, r ^ low],
            dst_ref=arrived.at[u, i, r],
            send_sem=row_send.at[r, u, i],
            recv_sem=row_recv.at[r, u, i],
            device_id={"tp": tp ^ low},
            device_id_type=MESH,
        )

    def start_down(first, last):
        @pl.loop(first, last)
        def _(j):
            for r in forwards[0]:
                down_copy(r, j).start()

    @pl.loop(0, D_CHUNKS)
    def _(j):
        down_copy(0, j).start()

    pl.semaphore_wait(barrier, n_ep - 1 + n_tp - 1)
    start_down(0, FIRST)

    for load in loads[:4]:
        load.wait()
    mine = pl.ds(aligned(tp, tokens), tokens)
    own = named[:, mine]
    own_share = shares[:, mine]
    top = own.shape[0]
    experts = lax.broadcasted_iota(jnp.int32, (n_ep, tokens), 0)
    onehot = [
        (experts == jnp.broadcast_to(own[k : k + 1, :], (n_ep, tokens))).astype(jnp.float32)
        for k in range(top)
    ]
    per_token = functools.reduce(lambda a, b: a + b, onehot)
    before = (
        lax.broadcasted_iota(jnp.int32, (tokens, tokens), 0)
        < lax.broadcasted_iota(jnp.int32, (tokens, tokens), 1)
    ).astype(jnp.bfloat16)
    earlier = jnp.dot(per_token.astype(jnp.bfloat16), before, preferred_element_type=jnp.float32)
    slot_rows = lax.broadcasted_iota(jnp.int32, (slots, tokens), 0)
    picked = jnp.zeros((slots, tokens), jnp.float32)
    spread = jnp.zeros((slots, tokens), jnp.float32)
    shift = sub.bit_length() - 1
    for k in range(top):
        rank = jnp.sum(onehot[k] * earlier, axis=0, keepdims=True).astype(jnp.int32)
        away = jnp.bitwise_xor(own[k : k + 1, :], ep)
        turn = lax.shift_right_logical(rank, jnp.full_like(rank, shift))
        far = jnp.where(away >= group, 1, 0)
        slot = ((far * rounds + turn) * group + away - far * group) * sub + rank - turn * sub
        match = slot_rows == jnp.broadcast_to(slot, (slots, tokens))
        picked = picked + jnp.where(match, 1.0, 0.0)
        spread = spread + jnp.where(
            match, jnp.broadcast_to(own_share[k : k + 1, :], (slots, tokens)), 0.0
        )
    picked = picked.reshape(2, rounds, group * sub, tokens).astype(jnp.bfloat16)
    for half in range(2):
        pick[:, half * group * sub : (half + 1) * group * sub, :] = picked[half]
    spread = spread.T
    high = spread.astype(jnp.bfloat16)
    low = (spread - high.astype(jnp.float32)).astype(jnp.bfloat16)
    for i, part in enumerate((high, low)):
        share_near[i] = part[:, : slots // 2]
        share_far[i] = part[:, slots // 2 :]
    share_copy = pltpu.make_async_remote_copy(
        src_ref=share_far,
        dst_ref=share_in.at[1 - inner],
        send_sem=share_send,
        recv_sem=share_recv.at[1 - inner],
        device_id={"ep": peer(group + quarter * inner)},
        device_id_type=MESH,
    )

    @pl.loop(0, tokens // NORM_ROWS)
    def _(i):
        at = aligned(i, NORM_ROWS)
        normed[pl.ds(at, NORM_ROWS), :] = norm_rows(x_in, e_gain, at)

    def send_rows(u, i):
        half = u // rounds
        return pltpu.make_async_remote_copy(
            src_ref=outgoing.at[u, i],
            dst_ref=arrived.at[u, i, 0],
            send_sem=out_send.at[u, i],
            recv_sem=out_recv.at[u, i],
            device_id={"ep": peer(half * group + i)},
            device_id_type=MESH,
        )

    sequence = [0, rounds] + list(range(1, rounds)) + list(range(rounds + 1, n_groups))

    def send_group(u):
        @pl.loop(0 if u >= rounds else 1, group)
        def _(i):
            send_rows(u, i).start()

    for k in range(rounds):
        rows = jnp.dot(pick[k], normed[...], preferred_element_type=jnp.float32)
        rows = rows.astype(jnp.bfloat16).reshape(2, group, sub, width)
        arrived[k, 0, 0] = rows[0, 0]
        for half in range(2):
            outgoing[half * rounds + k] = rows[half]
        for r in forwards[0]:
            row_copy(r, k, 0).start()
        for u in (0, rounds) if k == 0 else (k,):
            send_group(u)
    for u in range(rounds + 1, n_groups):
        send_group(u)
    share_copy.start()

    for load in loads[4:]:
        load.wait()

    @pl.loop(0, tokens // NORM_ROWS)
    def _(i):
        at = aligned(i, NORM_ROWS)
        rows = norm_rows(m_in, m_gain, at)
        for g in range(n_tp):
            m_normed[g, pl.ds(at, NORM_ROWS), :] = rows[:, g * group_width : (g + 1) * group_width]

    own_rows = pl.ds(pl.multiple_of(WMAX + tp * tokens, WMAX), tokens)
    m_rows[own_rows, :] = m_normed[tp]

    last = n_tp - 1

    def tail_copy(r):
        return pltpu.make_async_remote_copy(
            src_ref=m_normed.at[last ^ r, tokens - WMAX : tokens, :],
            dst_ref=m_tail,
            send_sem=tail_send.at[r],
            recv_sem=tail_recv,
            device_id={"tp": tp ^ r},
            device_id_type=MESH,
        )

    halo = pltpu.make_async_remote_copy(
        src_ref=m_tail,
        dst_ref=m_rows.at[0:WMAX, :],
        send_sem=halo_send,
        recv_sem=halo_recv,
        device_id={"ep": lax.rem(ep + 1, n_ep)},
        device_id_type=MESH,
    )

    @pl.when(tp == last)
    def _():
        for r in range(1, n_tp):
            tail_copy(r).start()
        m_tail[...] = m_normed[last, tokens - WMAX : tokens, :]


    def send_mix(r):
        return pltpu.make_async_remote_copy(
            src_ref=m_normed.at[tp ^ r],
            dst_ref=m_rows.at[own_rows, :],
            send_sem=mix_send.at[r],
            recv_sem=mix_recv.at[r],
            device_id={"tp": tp ^ r},
            device_id_type=MESH,
        )

    def take(u):
        @pl.loop(0 if u >= rounds else 1, group)
        def _(i):
            send_rows(u, i).wait_recv()
            for r in forwards[0]:
                row_copy(r, u, i).start()

    def relay(u):
        for r in relays:

            @pl.loop(0, group)
            def _(i):
                row_copy(r, u, i).wait_recv()
                for target in forwards[r]:
                    row_copy(target, u, i).start()

    def hid_copy(r, u):
        return pltpu.make_async_remote_copy(
            src_ref=hidden_out.at[u, r],
            dst_ref=hidden.at[u, :, :, r * part_units : (r + 1) * part_units],
            send_sem=hid_send.at[r, u],
            recv_sem=hid_recv.at[r, u],
            device_id={"tp": tp ^ r},
            device_id_type=MESH,
        )

    def work(u):
        for r in leaves:

            @pl.loop(0, group)
            def _(i):
                row_copy(r, u, i).wait_recv()

        @pl.loop(0, K_CHUNKS)
        def _(k):
            span = pl.ds(aligned(k, k_size), k_size)
            rows = arrived[u, :, :, :, span].reshape(group * n_tp * sub, k_size)
            product = jnp.dot(rows, gate_up[span, :], preferred_element_type=jnp.float32)

            @pl.when(k == 0)
            def _():
                acc[...] = product

            @pl.when(k > 0)
            def _():
                acc[...] += product

        units_of = clamped_unit(acc[:, :part_units], acc[:, part_units:])
        units_of = units_of.reshape(group, n_tp, sub, part_units)
        hidden[u, :, :, 0:part_units] = units_of[:, 0]
        for r in range(1, n_tp):
            hidden_out[u, r] = units_of[:, r]
            hid_copy(r, u).start()

    for step in range(len(sequence) + 2):
        if step < len(sequence):
            take(sequence[step])
        if step == min(1, len(sequence) - 1):

            @pl.when(tp != last)
            def _():
                tail_copy(1).wait_recv()

            halo.start()
        if step == len(sequence) and step >= 2:
            work(sequence[step - 2])
            start_down(FIRST, SECOND)
        if 1 <= step <= len(sequence):
            relay(sequence[step - 1])
        if step >= 2 and step != len(sequence) or step == len(sequence) + 1:
            work(sequence[step - 2])

    start_down(SECOND, D_CHUNKS)
    for r in range(1, n_tp):
        send_mix(r).start()

    for u in sequence:
        for r in range(1, n_tp):
            hid_copy(r, u).wait_recv()

    far = slice(rounds, n_groups)

    def send_back(j, i):
        return pltpu.make_async_remote_copy(
            src_ref=result.at[j, 0:rounds, i],
            dst_ref=returned.at[j, :, i],
            send_sem=ret_send.at[j, i],
            recv_sem=ret_recv.at[j, i],
            device_id={"ep": peer(i)},
            device_id_type=MESH,
        )

    def send_near(j):
        @pl.loop(1, group)
        def _(i):
            send_back(j, i).start()

    def bit_of(i):
        return lax.rem(lax.div(i, quarter), 2)

    def collect(j, i, kind, step):
        return pltpu.make_async_remote_copy(
            src_ref=result.at[j, far, i],
            dst_ref=gathered.at[kind, j, :, i],
            send_sem=col_send.at[j, i],
            recv_sem=col_recv.at[kind, j, i],
            device_id={"ep": peer(step)},
            device_id_type=MESH,
        )

    def collect_out(j, i):
        kind = jnp.bitwise_xor(bit_of(i), inner)
        step = lax.rem(i, quarter) + (1 - inner) * quarter
        return kind, step

    def collect_in(i, kind):
        return lax.rem(i, quarter) + (1 - jnp.bitwise_xor(bit_of(i), kind)) * quarter

    def partial_copy(kind, j):
        return pltpu.make_async_remote_copy(
            src_ref=partial_out.at[kind, j],
            dst_ref=partial_in.at[j],
            send_sem=part_send.at[kind, j],
            recv_sem=part_recv.at[j],
            device_id={"ep": peer(group + (1 - kind) * quarter)},
            device_id_type=MESH,
        )

    def sum_far(j):
        @pl.when(inner == 1)
        def _():
            for kind in (1, 0):

                @pl.loop(0, group)
                def _(i):
                    step = collect_in(i, kind)

                    @pl.when(step > 0)
                    def _():
                        collect(j, i, kind, step).wait_recv()

                rows = gathered[kind, j].reshape(slots // 2, d_size)
                partial_out[kind, j] = (
                    jnp.dot(share_in[kind, 0], rows, preferred_element_type=jnp.float32)
                    + jnp.dot(share_in[kind, 1], rows, preferred_element_type=jnp.float32)
                ).astype(jnp.bfloat16)
                partial_copy(kind, j).start()

    def down_arrive(j):
        down_copy(0, j).wait()
        for r in relays:
            down_copy(r, j).wait_recv()
            for target in forwards[r]:
                down_copy(target, j).start()
        for r in leaves:
            down_copy(r, j).wait_recv()

    @pl.when(inner == 1)
    def _():
        for kind in range(2):
            pltpu.make_async_remote_copy(
                src_ref=share_far,
                dst_ref=share_in.at[kind],
                send_sem=share_send,
                recv_sem=share_recv.at[kind],
                device_id={"ep": peer(group)},
                device_id_type=MESH,
            ).wait_recv()

    @pl.loop(0, D_CHUNKS)
    def _(j):
        down_arrive(j)
        weight = down_b[:, :, pl.ds(aligned(j, d_size), d_size)].reshape(units, d_size)
        rows = hidden[...].reshape(slots, units)
        product = jnp.dot(rows, weight, preferred_element_type=jnp.float32)
        result[j] = product.astype(jnp.bfloat16).reshape(n_groups, group, sub, d_size)

        @pl.loop(0, group)
        def _(i):
            kind, step = collect_out(j, i)

            @pl.when(step > 0)
            def _():
                collect(j, i, kind, step).start()

            @pl.when(step == 0)
            def _():
                gathered[kind, j, :, i] = result[j, far, i]

        returned[j, :, 0] = result[j, 0:rounds, 0]

        @pl.when(j >= near_lag)
        def _():
            send_near(j - near_lag)

        @pl.when(j >= lag)
        def _():
            sum_far(j - lag)

    @pl.loop(D_CHUNKS - near_lag, D_CHUNKS)
    def _(j):
        send_near(j)

    @pl.loop(D_CHUNKS - lag, D_CHUNKS)
    def _(j):
        sum_far(j)

    for r in range(1, n_tp):
        theirs = pl.ds(pl.multiple_of(WMAX + (tp ^ r) * tokens, WMAX), tokens)
        pltpu.make_async_remote_copy(
            src_ref=m_normed.at[tp ^ r],
            dst_ref=m_rows.at[theirs, :],
            send_sem=mix_send.at[r],
            recv_sem=mix_recv.at[r],
            device_id={"tp": tp ^ r},
            device_id_type=MESH,
        ).wait_recv()
    halo.wait_recv()
    window = 2 << tp
    span_rows = tokens + WMAX
    here = lax.broadcasted_iota(jnp.int32, (tokens, span_rows), 0)
    there = lax.broadcasted_iota(jnp.int32, (tokens, span_rows), 1)
    back = here + WMAX - there
    inside = (back >= 0) & (back < window)
    row = lax.broadcasted_iota(jnp.int32, (tokens, 1), 0)
    stores = []
    for b in range(n_tp):
        position = (ep * n_tp + b) * tokens
        band = (inside & (there + position >= WMAX)).astype(jnp.bfloat16)
        values = m_rows[b * tokens : b * tokens + span_rows, :]
        total = jnp.dot(band, values, preferred_element_type=jnp.float32)
        counts = jnp.minimum(row + position + 1, window).astype(jnp.float32)
        pooled = (total / counts - values[WMAX:, :].astype(jnp.float32)).astype(jnp.bfloat16)
        product = jnp.dot(pooled, g_weight[...], preferred_element_type=jnp.float32)
        m_out[b] = (product * scale[...]).astype(jnp.bfloat16)
        store = pltpu.make_async_copy(
            m_out.at[b], mixed_out.at[b * tokens : (b + 1) * tokens, :], m_store.at[b]
        )
        store.start()
        stores.append(store)

    def write_out(j):
        return pltpu.make_async_copy(
            e_out.at[j], expert_out.at[:, pl.ds(aligned(j, d_size), d_size)], e_store.at[j]
        )

    @pl.loop(0, D_CHUNKS)
    def _(j):
        @pl.loop(1, group)
        def _(i):
            send_back(j, i).wait_recv()

        partial_copy(0, j).wait_recv()
        rows = returned[j].reshape(slots // 2, d_size)
        e_out[j] = (
            jnp.dot(share_near[0], rows, preferred_element_type=jnp.float32)
            + jnp.dot(share_near[1], rows, preferred_element_type=jnp.float32)
            + partial_in[j].astype(jnp.float32)
        ).astype(jnp.bfloat16)
        write_out(j).start()

    for r in range(1, n_tp):

        @pl.loop(0, D_CHUNKS)
        def _(j):
            down_copy(r, j).wait_send()

        @pl.loop(0, n_groups)
        def _(u):
            hid_copy(r, u).wait_send()

        @pl.loop(0, n_groups)
        def _(u):
            @pl.loop(0, group)
            def _(i):
                row_copy(r, u, i).wait_send()

        send_mix(r).wait_send()
    halo.wait_send()

    @pl.when(tp == last)
    def _():
        for r in range(1, n_tp):
            tail_copy(r).wait_send()

    share_copy.wait_send()

    for half in range(2):

        @pl.loop(1 - half, group)
        def _(i):
            for u in range(half * rounds, (half + 1) * rounds):
                send_rows(u, i).wait_send()

    @pl.loop(0, D_CHUNKS)
    def _(j):
        @pl.loop(0, group)
        def _(i):
            kind, step = collect_out(j, i)

            @pl.when(step > 0)
            def _():
                collect(j, i, kind, step).wait_send()

        @pl.loop(1, group)
        def _(i):
            send_back(j, i).wait_send()

        @pl.when(inner == 1)
        def _():
            for kind in range(2):
                partial_copy(kind, j).wait_send()

    @pl.loop(0, D_CHUNKS)
    def _(j):
        write_out(j).wait()

    for store in stores:
        store.wait()


def shards(
    mixer_in,
    mixer_gain,
    group_weight,
    group_scale,
    expert_in,
    expert_gain,
    routes,
    route_weight,
    gate_weight,
    up_weight,
    down_weight,
):
    n_ep = lax.axis_size("ep")
    n_tp = lax.axis_size("tp")
    tokens, width = expert_in.shape
    group_width = group_weight.shape[-1]
    block_tokens, top = routes.shape
    part_units = gate_weight.shape[-1]
    units = part_units * n_tp
    capacity = max(2, 3 * tokens * top // (2 * n_ep))
    capacity = -(-capacity // 8) * 8
    slots = n_ep * capacity
    sub = 16 if capacity % 16 == 0 else 8
    rounds = capacity // sub
    groups = 2 * rounds
    group = n_ep // 2
    d_size = width // D_CHUNKS
    bf16, f32 = jnp.bfloat16, jnp.float32
    vmem = pltpu.VMEM
    dma = pltpu.SemaphoreType.DMA
    anywhere = pl.BlockSpec(memory_space=pl.ANY)
    scratch = [
        vmem((tokens, width), bf16),
        vmem((tokens, width), bf16),
        vmem((1, width), f32),
        vmem((1, width), f32),
        vmem((1, group_width), f32),
        vmem((top, block_tokens), jnp.int32),
        vmem((top, block_tokens), f32),
        vmem((width, 2 * part_units), bf16),
        vmem((n_tp, part_units, width), bf16),
        vmem((tokens, width), bf16),
        vmem((rounds, n_ep * sub, tokens), bf16),
        vmem((2, tokens, slots // 2), bf16),
        vmem((2, tokens, slots // 2), bf16),
        vmem((2, 2, tokens, slots // 2), bf16),
        vmem((groups, group, sub, width), bf16),
        vmem((groups, group, n_tp, sub, width), bf16),
        vmem((group * n_tp * sub, 2 * part_units), f32),
        vmem((groups, n_tp, group, sub, part_units), bf16),
        vmem((groups, group, sub, units), bf16),
        vmem((D_CHUNKS, groups, group, sub, d_size), bf16),
        vmem((D_CHUNKS, rounds, group, sub, d_size), bf16),
        vmem((2, D_CHUNKS, rounds, group, sub, d_size), bf16),
        vmem((2, D_CHUNKS, tokens, d_size), bf16),
        vmem((D_CHUNKS, tokens, d_size), bf16),
        vmem((n_tp, tokens, group_width), bf16),
        vmem((WMAX + n_tp * tokens, group_width), bf16),
        vmem((WMAX, group_width), bf16),
        vmem((group_width, group_width), bf16),
        vmem((n_tp, tokens, group_width), bf16),
        vmem((D_CHUNKS, tokens, d_size), bf16),
        dma((10,)),
        dma((n_tp, D_CHUNKS)),
        dma((n_tp, D_CHUNKS)),
        dma((groups, group)),
        dma((groups, group)),
        dma((n_tp, groups, group)),
        dma((n_tp, groups, group)),
        dma((n_tp, groups)),
        dma((n_tp, groups)),
        dma((D_CHUNKS, group)),
        dma((D_CHUNKS, group)),
        dma(()),
        dma((2,)),
        dma((D_CHUNKS, group)),
        dma((2, D_CHUNKS, group)),
        dma((2, D_CHUNKS)),
        dma((D_CHUNKS,)),
        dma((n_tp,)),
        dma((n_tp,)),
        dma((n_tp,)),
        dma(()),
        dma(()),
        dma(()),
        dma((n_tp,)),
        dma((D_CHUNKS,)),
    ]
    flops = 6 * slots * width * units + 2 * n_tp * tokens * group_width * group_width
    return pl.pallas_call(
        functools.partial(kernel, n_ep, n_tp),
        out_shape=(
            jax.ShapeDtypeStruct((n_tp * tokens, group_width), bf16),
            jax.ShapeDtypeStruct((tokens, width), bf16),
        ),
        in_specs=[anywhere] * 11,
        out_specs=(anywhere, anywhere),
        scratch_shapes=scratch,
        compiler_params=pltpu.CompilerParams(
            collective_id=0, has_side_effects=True, vmem_limit_bytes=67043328
        ),
        cost_estimate=pl.CostEstimate(flops=flops, bytes_accessed=1 << 26, transcendentals=0),
    )(
        mixer_in,
        mixer_gain.reshape(1, width),
        group_weight,
        group_scale,
        expert_in,
        expert_gain.reshape(1, width),
        routes.T,
        route_weight.T,
        gate_weight,
        up_weight,
        down_weight,
    )


def solution(mesh):
    in_specs = (
        P(("ep", "tp"), None),
        P(),
        P("tp", None, None),
        P("tp", None),
        P(("ep", "tp"), None),
        P(),
        P("ep", None),
        P("ep", None),
        P("ep", None, "tp"),
        P("ep", None, "tp"),
        P("ep", "tp", None),
    )
    out_specs = (P("ep", "tp"), P(("ep", "tp"), None))
    return jax.shard_map(shards, mesh=mesh, in_specs=in_specs, out_specs=out_specs, check_vma=False)
```

```python
import functools
import jax
import jax.numpy as jnp
from jax import lax
from jax.experimental import pallas as pl
from jax.experimental.pallas import tpu as pltpu
from jax.sharding import PartitionSpec as P

WMAX = 16
NORM_ROWS = 16
K_CHUNKS = 8
D_CHUNKS = 16
FIRST = 1
SECOND = 2

epsilon = 1e-06
clamp_limit = 7.0
sigmoid_slope = 1.702

MESH = pl.DeviceIdType.MESH


def clamped_unit(gate_part, up_part):
    gate_part = jnp.minimum(gate_part, clamp_limit)
    up_part = jnp.clip(up_part, -clamp_limit, clamp_limit)
    return ((up_part + 1.0) * gate_part * jax.nn.sigmoid(sigmoid_slope * gate_part)).astype(
        jnp.bfloat16
    )


def norm_rows(source, gain, at):
    widened = source[pl.ds(at, NORM_ROWS), :].astype(jnp.float32)
    mean = jnp.sum(widened * widened, axis=-1, keepdims=True) * (1.0 / widened.shape[-1])
    return (widened * lax.rsqrt(mean + epsilon) * gain[...]).astype(jnp.bfloat16)


def aligned(value, size):
    return pl.multiple_of(value * size, size)


def kernel(
    n_ep,
    n_tp,
    mixer_in,
    mixer_gain,
    group_weight,
    group_scale,
    expert_in,
    expert_gain,
    routes,
    route_weight,
    gate_w,
    up_w,
    down_w,
    mixed_out,
    expert_out,
    x_in,
    m_in,
    e_gain,
    m_gain,
    scale,
    named,
    shares,
    gate_up,
    down_b,
    normed,
    pick,
    share_near,
    share_far,
    share_in,
    outgoing,
    arrived,
    acc,
    hidden_out,
    hidden,
    result,
    returned,
    gathered,
    partial_out,
    partial_in,
    m_normed,
    m_rows,
    m_tail,
    g_weight,
    m_out,
    e_out,
    load_sem,
    down_send,
    down_recv,
    out_send,
    out_recv,
    row_send,
    row_recv,
    leaf_recv,
    hid_send,
    hid_recv,
    ret_send,
    ret_recv,
    share_send,
    share_recv,
    col_send,
    col_recv,
    part_send,
    part_recv,
    mix_send,
    mix_recv,
    tail_send,
    tail_recv,
    halo_send,
    halo_recv,
    m_store,
    e_store,
):
    ep = lax.axis_index("ep")
    tp = lax.axis_index("tp")
    tokens, width = x_in.shape
    group_width = g_weight.shape[0]
    n_groups, group, sub, units = hidden.shape
    rounds = n_groups // 2
    slots = n_ep * rounds * sub
    quarter = n_ep // 4
    lag = 2
    near_lag = 4
    part_units = units // n_tp
    k_size = width // K_CHUNKS
    d_size = width // D_CHUNKS

    def peer(i):
        return jnp.bitwise_xor(ep, i)

    inner = jnp.bitwise_xor(lax.rem(lax.div(ep, quarter), 2), lax.div(ep, group))

    loads = [
        pltpu.make_async_copy(origin, target, load_sem.at[i])
        for i, (origin, target) in enumerate(
            [
                (expert_in, x_in),
                (expert_gain, e_gain),
                (routes, named),
                (route_weight, shares),
                (gate_w.at[0], gate_up.at[:, 0:part_units]),
                (up_w.at[0], gate_up.at[:, part_units : 2 * part_units]),
                (mixer_in, m_in),
                (mixer_gain, m_gain),
                (group_scale, scale),
                (group_weight.at[0], g_weight),
            ]
        )
    ]
    for load in loads:
        load.start()

    barrier = pltpu.get_barrier_semaphore()
    for r in range(1, n_tp):
        pl.semaphore_signal(barrier, inc=1, device_id={"tp": tp ^ r}, device_id_type=MESH)

    @pl.loop(1, n_ep)
    def _(i):
        pl.semaphore_signal(barrier, inc=1, device_id={"ep": peer(i)}, device_id_type=MESH)

    bits = []
    while (1 << len(bits)) < n_tp:
        bits.insert(0, 1 << len(bits))
    forwards = {r: [r | b for b in bits if r == 0 or b < (r & -r)] for r in range(n_tp)}
    order = [0] + sorted(range(1, n_tp), key=lambda r: (r & (n_tp // 2) > 0, bin(r).count("1")))
    relays = [r for r in order[1:] if forwards[r]]
    leaves = [r for r in order[1:] if not forwards[r]]

    def down_copy(r, j):
        low = r & -r
        span = (slice(None), pl.ds(aligned(j, d_size), d_size))
        origin = down_w.at[(0,) + span] if r == low else down_b.at[(r ^ low,) + span]
        if r == 0:
            return pltpu.make_async_copy(origin, down_b.at[(0,) + span], down_recv.at[0, j])
        return pltpu.make_async_remote_copy(
            src_ref=origin,
            dst_ref=down_b.at[(r,) + span],
            send_sem=down_send.at[r],
            recv_sem=down_recv.at[r, j],
            device_id={"tp": tp ^ low},
            device_id_type=MESH,
        )

    def row_copy(r, u, i):
        low = r & -r
        return pltpu.make_async_remote_copy(
            src_ref=arrived.at[u, i, r ^ low],
            dst_ref=arrived.at[u, i, r],
            send_sem=row_send.at[r],
            recv_sem=row_recv.at[relays.index(r), u, i] if r in relays else leaf_recv.at[r, u],
            device_id={"tp": tp ^ low},
            device_id_type=MESH,
        )

    def everything(ref, send, recv):
        return pltpu.make_async_remote_copy(
            src_ref=ref,
            dst_ref=ref,
            send_sem=send,
            recv_sem=recv,
            device_id={"ep": peer(1)},
            device_id_type=MESH,
        )

    def start_down(first, last):
        @pl.loop(first, last)
        def _(j):
            for r in forwards[0]:
                down_copy(r, j).start()

    @pl.loop(0, D_CHUNKS)
    def _(j):
        down_copy(0, j).start()

    pl.semaphore_wait(barrier, n_ep - 1 + n_tp - 1)
    start_down(0, FIRST)

    for load in loads[:4]:
        load.wait()
    mine = pl.ds(aligned(tp, tokens), tokens)
    own = named[:, mine]
    own_share = shares[:, mine]
    top = own.shape[0]
    experts = lax.broadcasted_iota(jnp.int32, (n_ep, tokens), 0)
    onehot = [
        (experts == jnp.broadcast_to(own[k : k + 1, :], (n_ep, tokens))).astype(jnp.float32)
        for k in range(top)
    ]
    per_token = functools.reduce(lambda a, b: a + b, onehot)
    before = (
        lax.broadcasted_iota(jnp.int32, (tokens, tokens), 0)
        < lax.broadcasted_iota(jnp.int32, (tokens, tokens), 1)
    ).astype(jnp.bfloat16)
    earlier = jnp.dot(per_token.astype(jnp.bfloat16), before, preferred_element_type=jnp.float32)
    slot_rows = lax.broadcasted_iota(jnp.int32, (slots, tokens), 0)
    picked = jnp.zeros((slots, tokens), jnp.float32)
    spread = jnp.zeros((slots, tokens), jnp.float32)
    shift = sub.bit_length() - 1
    for k in range(top):
        rank = jnp.sum(onehot[k] * earlier, axis=0, keepdims=True).astype(jnp.int32)
        away = jnp.bitwise_xor(own[k : k + 1, :], ep)
        turn = lax.shift_right_logical(rank, jnp.full_like(rank, shift))
        far = jnp.where(away >= group, 1, 0)
        slot = ((far * rounds + turn) * group + away - far * group) * sub + rank - turn * sub
        match = slot_rows == jnp.broadcast_to(slot, (slots, tokens))
        picked = picked + jnp.where(match, 1.0, 0.0)
        spread = spread + jnp.where(
            match, jnp.broadcast_to(own_share[k : k + 1, :], (slots, tokens)), 0.0
        )
    picked = picked.reshape(2, rounds, group * sub, tokens).astype(jnp.bfloat16)
    for half in range(2):
        pick[:, half * group * sub : (half + 1) * group * sub, :] = picked[half]
    spread = spread.T
    high = spread.astype(jnp.bfloat16)
    low = (spread - high.astype(jnp.float32)).astype(jnp.bfloat16)
    for i, part in enumerate((high, low)):
        share_near[i] = part[:, : slots // 2]
        share_far[i] = part[:, slots // 2 :]
    share_copy = pltpu.make_async_remote_copy(
        src_ref=share_far,
        dst_ref=share_in.at[1 - inner],
        send_sem=share_send,
        recv_sem=share_recv.at[1 - inner],
        device_id={"ep": peer(group + quarter * inner)},
        device_id_type=MESH,
    )

    @pl.loop(0, tokens // NORM_ROWS)
    def _(i):
        at = aligned(i, NORM_ROWS)
        normed[pl.ds(at, NORM_ROWS), :] = norm_rows(x_in, e_gain, at)

    def send_rows(u, i):
        half = u // rounds
        return pltpu.make_async_remote_copy(
            src_ref=outgoing.at[u, i],
            dst_ref=arrived.at[u, i, 0],
            send_sem=out_send.at[half, i],
            recv_sem=out_recv.at[u, i],
            device_id={"ep": peer(half * group + i)},
            device_id_type=MESH,
        )

    sequence = [0, rounds] + list(range(1, rounds)) + list(range(rounds + 1, n_groups))

    def send_group(u):
        @pl.loop(0 if u >= rounds else 1, group)
        def _(i):
            send_rows(u, i).start()

    for k in range(rounds):
        rows = jnp.dot(pick[k], normed[...], preferred_element_type=jnp.float32)
        rows = rows.astype(jnp.bfloat16).reshape(2, group, sub, width)
        arrived[k, 0, 0] = rows[0, 0]
        for half in range(2):
            outgoing[half * rounds + k] = rows[half]
        for r in forwards[0]:
            row_copy(r, k, 0).start()
        for u in (0, rounds) if k == 0 else (k,):
            send_group(u)
    for u in range(rounds + 1, n_groups):
        send_group(u)

    for load in loads[4:]:
        load.wait()

    @pl.loop(0, tokens // NORM_ROWS)
    def _(i):
        at = aligned(i, NORM_ROWS)
        rows = norm_rows(m_in, m_gain, at)
        for g in range(n_tp):
            m_normed[g, pl.ds(at, NORM_ROWS), :] = rows[:, g * group_width : (g + 1) * group_width]

    own_rows = pl.ds(pl.multiple_of(WMAX + tp * tokens, WMAX), tokens)
    m_rows[own_rows, :] = m_normed[tp]

    last = n_tp - 1

    def tail_copy(r):
        return pltpu.make_async_remote_copy(
            src_ref=m_normed.at[last ^ r, tokens - WMAX : tokens, :],
            dst_ref=m_tail,
            send_sem=tail_send.at[r],
            recv_sem=tail_recv,
            device_id={"tp": tp ^ r},
            device_id_type=MESH,
        )

    halo = pltpu.make_async_remote_copy(
        src_ref=m_tail,
        dst_ref=m_rows.at[0:WMAX, :],
        send_sem=halo_send,
        recv_sem=halo_recv,
        device_id={"ep": lax.rem(ep + 1, n_ep)},
        device_id_type=MESH,
    )

    @pl.when(tp == last)
    def _():
        for r in range(1, n_tp):
            tail_copy(r).start()
        m_tail[...] = m_normed[last, tokens - WMAX : tokens, :]


    def send_mix(r):
        return pltpu.make_async_remote_copy(
            src_ref=m_normed.at[tp ^ r],
            dst_ref=m_rows.at[own_rows, :],
            send_sem=mix_send.at[r],
            recv_sem=mix_recv.at[r],
            device_id={"tp": tp ^ r},
            device_id_type=MESH,
        )

    def take(u):
        @pl.loop(0 if u >= rounds else 1, group)
        def _(i):
            send_rows(u, i).wait_recv()
            for r in forwards[0]:
                row_copy(r, u, i).start()

    def relay(u):
        for r in relays:

            @pl.loop(0, group)
            def _(i):
                row_copy(r, u, i).wait_recv()
                for target in forwards[r]:
                    row_copy(target, u, i).start()

    def hid_copy(r, u):
        return pltpu.make_async_remote_copy(
            src_ref=hidden_out.at[u, r],
            dst_ref=hidden.at[u, :, :, r * part_units : (r + 1) * part_units],
            send_sem=hid_send.at[r],
            recv_sem=hid_recv.at[r],
            device_id={"tp": tp ^ r},
            device_id_type=MESH,
        )

    def work(u):
        for r in leaves:
            everything(arrived.at[u, :, r], row_send.at[r], leaf_recv.at[r, u]).wait_recv()

        @pl.loop(0, K_CHUNKS)
        def _(k):
            span = pl.ds(aligned(k, k_size), k_size)
            rows = arrived[u, :, :, :, span].reshape(group * n_tp * sub, k_size)
            product = jnp.dot(rows, gate_up[span, :], preferred_element_type=jnp.float32)

            @pl.when(k == 0)
            def _():
                acc[...] = product

            @pl.when(k > 0)
            def _():
                acc[...] += product

        units_of = clamped_unit(acc[:, :part_units], acc[:, part_units:])
        units_of = units_of.reshape(group, n_tp, sub, part_units)
        hidden[u, :, :, 0:part_units] = units_of[:, 0]
        for r in range(1, n_tp):
            hidden_out[u, r] = units_of[:, r]
            hid_copy(r, u).start()

    for step in range(len(sequence) + 2):
        if step < len(sequence):
            take(sequence[step])
        if step == min(1, len(sequence) - 1):

            @pl.when(tp != last)
            def _():
                tail_copy(1).wait_recv()

            halo.start()
        if step == len(sequence):
            share_copy.start()
        if step == len(sequence) and step >= 2:
            work(sequence[step - 2])
            start_down(FIRST, SECOND)
        if 1 <= step <= len(sequence):
            relay(sequence[step - 1])
        if step >= 2 and step != len(sequence) or step == len(sequence) + 1:
            work(sequence[step - 2])

    start_down(SECOND, D_CHUNKS)
    for r in range(1, n_tp):
        send_mix(r).start()

    for r in range(1, n_tp):
        mine = hidden.at[:, :, :, r * part_units : (r + 1) * part_units]
        everything(mine, hid_send.at[r], hid_recv.at[r]).wait_recv()

    far = slice(rounds, n_groups)

    def send_back(j, i):
        return pltpu.make_async_remote_copy(
            src_ref=result.at[j, 0:rounds, i],
            dst_ref=returned.at[j, :, i],
            send_sem=ret_send.at[i],
            recv_sem=ret_recv.at[j],
            device_id={"ep": peer(i)},
            device_id_type=MESH,
        )

    def send_near(j):
        @pl.loop(1, group)
        def _(i):
            send_back(j, i).start()

    def bit_of(i):
        return lax.rem(lax.div(i, quarter), 2)

    def collect(j, i, kind, step):
        return pltpu.make_async_remote_copy(
            src_ref=result.at[j, far, i],
            dst_ref=gathered.at[kind, j, :, i],
            send_sem=col_send.at[i],
            recv_sem=col_recv.at[kind, j],
            device_id={"ep": peer(step)},
            device_id_type=MESH,
        )

    def collect_out(j, i):
        kind = jnp.bitwise_xor(bit_of(i), inner)
        step = lax.rem(i, quarter) + (1 - inner) * quarter
        return kind, step

    def partial_copy(kind, j):
        return pltpu.make_async_remote_copy(
            src_ref=partial_out.at[kind, j],
            dst_ref=partial_in.at[j],
            send_sem=part_send.at[kind],
            recv_sem=part_recv.at[j],
            device_id={"ep": peer(group + (1 - kind) * quarter)},
            device_id_type=MESH,
        )

    def sum_far(j):
        @pl.when(inner == 1)
        def _():
            for kind in (1, 0):

                several = gathered.at[kind, j, :, 0 : group - 1]
                everything(several, col_send.at[0], col_recv.at[kind, j]).wait_recv()
                rows = gathered[kind, j].reshape(slots // 2, d_size)
                partial_out[kind, j] = (
                    jnp.dot(share_in[kind, 0], rows, preferred_element_type=jnp.float32)
                    + jnp.dot(share_in[kind, 1], rows, preferred_element_type=jnp.float32)
                ).astype(jnp.bfloat16)
                partial_copy(kind, j).start()

    def down_arrive(j):
        down_copy(0, j).wait()
        for r in relays:
            down_copy(r, j).wait_recv()
            for target in forwards[r]:
                down_copy(target, j).start()
        for r in leaves:
            down_copy(r, j).wait_recv()

    @pl.when(inner == 1)
    def _():
        for kind in range(2):
            pltpu.make_async_remote_copy(
                src_ref=share_far,
                dst_ref=share_in.at[kind],
                send_sem=share_send,
                recv_sem=share_recv.at[kind],
                device_id={"ep": peer(group)},
                device_id_type=MESH,
            ).wait_recv()

    @pl.loop(0, D_CHUNKS)
    def _(j):
        down_arrive(j)
        weight = down_b[:, :, pl.ds(aligned(j, d_size), d_size)].reshape(units, d_size)
        rows = hidden[...].reshape(slots, units)
        product = jnp.dot(rows, weight, preferred_element_type=jnp.float32)
        result[j] = product.astype(jnp.bfloat16).reshape(n_groups, group, sub, d_size)

        @pl.loop(0, group)
        def _(i):
            kind, step = collect_out(j, i)

            @pl.when(step > 0)
            def _():
                collect(j, i, kind, step).start()

            @pl.when(step == 0)
            def _():
                gathered[kind, j, :, i] = result[j, far, i]

        returned[j, :, 0] = result[j, 0:rounds, 0]

        @pl.when(j >= near_lag)
        def _():
            send_near(j - near_lag)

        @pl.when(j >= lag)
        def _():
            sum_far(j - lag)

    @pl.loop(D_CHUNKS - near_lag, D_CHUNKS)
    def _(j):
        send_near(j)

    @pl.loop(D_CHUNKS - lag, D_CHUNKS)
    def _(j):
        sum_far(j)

    for r in range(1, n_tp):
        theirs = pl.ds(pl.multiple_of(WMAX + (tp ^ r) * tokens, WMAX), tokens)
        pltpu.make_async_remote_copy(
            src_ref=m_normed.at[tp ^ r],
            dst_ref=m_rows.at[theirs, :],
            send_sem=mix_send.at[r],
            recv_sem=mix_recv.at[r],
            device_id={"tp": tp ^ r},
            device_id_type=MESH,
        ).wait_recv()
    halo.wait_recv()
    window = 2 << tp
    span_rows = tokens + WMAX
    here = lax.broadcasted_iota(jnp.int32, (tokens, span_rows), 0)
    there = lax.broadcasted_iota(jnp.int32, (tokens, span_rows), 1)
    back = here + WMAX - there
    inside = (back >= 0) & (back < window)
    row = lax.broadcasted_iota(jnp.int32, (tokens, 1), 0)
    stores = []
    for b in range(n_tp):
        position = (ep * n_tp + b) * tokens
        band = (inside & (there + position >= WMAX)).astype(jnp.bfloat16)
        values = m_rows[b * tokens : b * tokens + span_rows, :]
        total = jnp.dot(band, values, preferred_element_type=jnp.float32)
        counts = jnp.minimum(row + position + 1, window).astype(jnp.float32)
        pooled = (total / counts - values[WMAX:, :].astype(jnp.float32)).astype(jnp.bfloat16)
        product = jnp.dot(pooled, g_weight[...], preferred_element_type=jnp.float32)
        m_out[b] = (product * scale[...]).astype(jnp.bfloat16)
        store = pltpu.make_async_copy(
            m_out.at[b], mixed_out.at[b * tokens : (b + 1) * tokens, :], m_store.at[b]
        )
        store.start()
        stores.append(store)

    def write_out(j):
        return pltpu.make_async_copy(
            e_out.at[j], expert_out.at[:, pl.ds(aligned(j, d_size), d_size)], e_store
        )

    @pl.loop(0, D_CHUNKS)
    def _(j):
        everything(returned.at[j, :, 1:group], ret_send.at[0], ret_recv.at[j]).wait_recv()
        partial_copy(0, j).wait_recv()
        rows = returned[j].reshape(slots // 2, d_size)
        e_out[j] = (
            jnp.dot(share_near[0], rows, preferred_element_type=jnp.float32)
            + jnp.dot(share_near[1], rows, preferred_element_type=jnp.float32)
            + partial_in[j].astype(jnp.float32)
        ).astype(jnp.bfloat16)
        write_out(j).start()

    for r in range(1, n_tp):
        everything(down_b.at[r], down_send.at[r], down_recv.at[r, 0]).wait_send()
        everything(hidden_out.at[:, r], hid_send.at[r], hid_recv.at[r]).wait_send()
        everything(arrived.at[:, :, r], row_send.at[r], hid_recv.at[r]).wait_send()
        send_mix(r).wait_send()
    halo.wait_send()
    share_copy.wait_send()

    @pl.when(tp == last)
    def _():
        for r in range(1, n_tp):
            tail_copy(r).wait_send()

    for half in range(2):
        rows_of = slice(half * rounds, (half + 1) * rounds)

        @pl.loop(1 - half, group)
        def _(i):
            everything(outgoing.at[rows_of, i], out_send.at[half, i], share_send).wait_send()

    @pl.loop(1, group)
    def _(i):
        everything(result.at[:, 0:rounds, i], ret_send.at[i], share_send).wait_send()

    @pl.loop(0, group)
    def _(i):
        _, step = collect_out(0, i)

        @pl.when(step > 0)
        def _():
            everything(result.at[:, far, i], col_send.at[i], share_send).wait_send()

    @pl.when(inner == 1)
    def _():
        for kind in range(2):
            everything(partial_out.at[kind], part_send.at[kind], share_send).wait_send()

    everything(e_out, share_send, e_store).wait_recv()
    for store in stores:
        store.wait()


def shards(
    mixer_in,
    mixer_gain,
    group_weight,
    group_scale,
    expert_in,
    expert_gain,
    routes,
    route_weight,
    gate_weight,
    up_weight,
    down_weight,
):
    n_ep = lax.axis_size("ep")
    n_tp = lax.axis_size("tp")
    tokens, width = expert_in.shape
    group_width = group_weight.shape[-1]
    block_tokens, top = routes.shape
    part_units = gate_weight.shape[-1]
    units = part_units * n_tp
    capacity = max(2, 3 * tokens * top // (2 * n_ep))
    capacity = -(-capacity // 8) * 8
    slots = n_ep * capacity
    sub = 16 if capacity % 16 == 0 else 8
    rounds = capacity // sub
    groups = 2 * rounds
    group = n_ep // 2
    d_size = width // D_CHUNKS
    bf16, f32 = jnp.bfloat16, jnp.float32
    vmem = pltpu.VMEM
    dma = pltpu.SemaphoreType.DMA
    anywhere = pl.BlockSpec(memory_space=pl.ANY)
    scratch = [
        vmem((tokens, width), bf16),
        vmem((tokens, width), bf16),
        vmem((1, width), f32),
        vmem((1, width), f32),
        vmem((1, group_width), f32),
        vmem((top, block_tokens), jnp.int32),
        vmem((top, block_tokens), f32),
        vmem((width, 2 * part_units), bf16),
        vmem((n_tp, part_units, width), bf16),
        vmem((tokens, width), bf16),
        vmem((rounds, n_ep * sub, tokens), bf16),
        vmem((2, tokens, slots // 2), bf16),
        vmem((2, tokens, slots // 2), bf16),
        vmem((2, 2, tokens, slots // 2), bf16),
        vmem((groups, group, sub, width), bf16),
        vmem((groups, group, n_tp, sub, width), bf16),
        vmem((group * n_tp * sub, 2 * part_units), f32),
        vmem((groups, n_tp, group, sub, part_units), bf16),
        vmem((groups, group, sub, units), bf16),
        vmem((D_CHUNKS, groups, group, sub, d_size), bf16),
        vmem((D_CHUNKS, rounds, group, sub, d_size), bf16),
        vmem((2, D_CHUNKS, rounds, group, sub, d_size), bf16),
        vmem((2, D_CHUNKS, tokens, d_size), bf16),
        vmem((D_CHUNKS, tokens, d_size), bf16),
        vmem((n_tp, tokens, group_width), bf16),
        vmem((WMAX + n_tp * tokens, group_width), bf16),
        vmem((WMAX, group_width), bf16),
        vmem((group_width, group_width), bf16),
        vmem((n_tp, tokens, group_width), bf16),
        vmem((D_CHUNKS, tokens, d_size), bf16),
        dma((10,)),
        dma((n_tp,)),
        dma((n_tp, D_CHUNKS)),
        dma((2, group)),
        dma((groups, group)),
        dma((n_tp,)),
        dma((max(1, n_tp // 2 - 1), groups, group)),
        dma((n_tp, groups)),
        dma((n_tp,)),
        dma((n_tp,)),
        dma((group,)),
        dma((D_CHUNKS,)),
        dma(()),
        dma((2,)),
        dma((group,)),
        dma((2, D_CHUNKS)),
        dma((2,)),
        dma((D_CHUNKS,)),
        dma((n_tp,)),
        dma((n_tp,)),
        dma((n_tp,)),
        dma(()),
        dma(()),
        dma(()),
        dma((n_tp,)),
        dma(()),
    ]
    flops = 6 * slots * width * units + 2 * n_tp * tokens * group_width * group_width
    return pl.pallas_call(
        functools.partial(kernel, n_ep, n_tp),
        out_shape=(
            jax.ShapeDtypeStruct((n_tp * tokens, group_width), bf16),
            jax.ShapeDtypeStruct((tokens, width), bf16),
        ),
        in_specs=[anywhere] * 11,
        out_specs=(anywhere, anywhere),
        scratch_shapes=scratch,
        compiler_params=pltpu.CompilerParams(
            collective_id=0, has_side_effects=True, vmem_limit_bytes=67043328
        ),
        cost_estimate=pl.CostEstimate(flops=flops, bytes_accessed=1 << 26, transcendentals=0),
    )(
        mixer_in,
        mixer_gain.reshape(1, width),
        group_weight,
        group_scale,
        expert_in,
        expert_gain.reshape(1, width),
        routes.T,
        route_weight.T,
        gate_weight,
        up_weight,
        down_weight,
    )


def solution(mesh):
    in_specs = (
        P(("ep", "tp"), None),
        P(),
        P("tp", None, None),
        P("tp", None),
        P(("ep", "tp"), None),
        P(),
        P("ep", None),
        P("ep", None),
        P("ep", None, "tp"),
        P("ep", None, "tp"),
        P("ep", "tp", None),
    )
    out_specs = (P("ep", "tp"), P(("ep", "tp"), None))
    return jax.shard_map(shards, mesh=mesh, in_specs=in_specs, out_specs=out_specs, check_vma=False)
```

```python
import functools
import jax
import jax.numpy as jnp
from jax import lax
from jax.experimental import pallas as pl
from jax.experimental.pallas import tpu as pltpu
from jax.sharding import PartitionSpec as P

WMAX = 16
NORM_ROWS = 16
K_CHUNKS = 1
D_CHUNKS = 16
FIRST = 1
SECOND = 2

epsilon = 1e-06
clamp_limit = 7.0
sigmoid_slope = 1.702

MESH = pl.DeviceIdType.MESH


def clamped_unit(gate_part, up_part):
    gate_part = jnp.minimum(gate_part, clamp_limit)
    up_part = jnp.clip(up_part, -clamp_limit, clamp_limit)
    return ((up_part + 1.0) * gate_part * jax.nn.sigmoid(sigmoid_slope * gate_part)).astype(
        jnp.bfloat16
    )


def norm_rows(source, gain, at):
    widened = source[pl.ds(at, NORM_ROWS), :].astype(jnp.float32)
    mean = jnp.sum(widened * widened, axis=-1, keepdims=True) * (1.0 / widened.shape[-1])
    return (widened * lax.rsqrt(mean + epsilon) * gain[...]).astype(jnp.bfloat16)


def aligned(value, size):
    return pl.multiple_of(value * size, size)


def kernel(
    n_ep,
    n_tp,
    mixer_in,
    mixer_gain,
    group_weight,
    group_scale,
    expert_in,
    expert_gain,
    routes,
    route_weight,
    gate_w,
    up_w,
    down_w,
    mixed_out,
    expert_out,
    x_in,
    m_in,
    e_gain,
    m_gain,
    scale,
    named,
    shares,
    gate_up,
    down_b,
    normed,
    pick,
    share_near,
    share_far,
    share_in,
    outgoing,
    arrived,
    acc,
    hidden_out,
    hidden,
    result,
    returned,
    gathered,
    partial_out,
    partial_in,
    m_normed,
    m_rows,
    m_tail,
    g_weight,
    m_out,
    e_out,
    load_sem,
    down_send,
    down_recv,
    out_send,
    out_recv,
    row_send,
    row_recv,
    leaf_recv,
    hid_send,
    hid_recv,
    ret_send,
    ret_recv,
    share_send,
    share_recv,
    col_send,
    col_recv,
    part_send,
    part_recv,
    mix_send,
    mix_recv,
    tail_send,
    tail_recv,
    halo_send,
    halo_recv,
    m_store,
    e_store,
):
    ep = lax.axis_index("ep")
    tp = lax.axis_index("tp")
    tokens, width = x_in.shape
    group_width = g_weight.shape[0]
    n_groups, group, sub, units = hidden.shape
    rounds = n_groups // 2
    slots = n_ep * rounds * sub
    quarter = n_ep // 4
    lag = 2
    near_lag = 4
    part_units = units // n_tp
    k_size = width // K_CHUNKS
    d_size = width // D_CHUNKS

    def peer(i):
        return jnp.bitwise_xor(ep, i)

    inner = jnp.bitwise_xor(lax.rem(lax.div(ep, quarter), 2), lax.div(ep, group))

    loads = [
        pltpu.make_async_copy(origin, target, load_sem.at[i])
        for i, (origin, target) in enumerate(
            [
                (expert_in, x_in),
                (expert_gain, e_gain),
                (routes, named),
                (route_weight, shares),
                (gate_w.at[0], gate_up.at[:, 0:part_units]),
                (up_w.at[0], gate_up.at[:, part_units : 2 * part_units]),
                (mixer_in, m_in),
                (mixer_gain, m_gain),
                (group_scale, scale),
                (group_weight.at[0], g_weight),
            ]
        )
    ]
    for load in loads:
        load.start()

    barrier = pltpu.get_barrier_semaphore()
    for r in range(1, n_tp):
        pl.semaphore_signal(barrier, inc=1, device_id={"tp": tp ^ r}, device_id_type=MESH)

    @pl.loop(1, n_ep)
    def _(i):
        pl.semaphore_signal(barrier, inc=1, device_id={"ep": peer(i)}, device_id_type=MESH)

    bits = []
    while (1 << len(bits)) < n_tp:
        bits.insert(0, 1 << len(bits))
    forwards = {r: [r | b for b in bits if r == 0 or b < (r & -r)] for r in range(n_tp)}
    order = [0] + sorted(range(1, n_tp), key=lambda r: (r & (n_tp // 2) > 0, bin(r).count("1")))
    relays = [r for r in order[1:] if forwards[r]]
    leaves = [r for r in order[1:] if not forwards[r]]

    def down_copy(r, j):
        low = r & -r
        span = (slice(None), pl.ds(aligned(j, d_size), d_size))
        origin = down_w.at[(0,) + span] if r == low else down_b.at[(r ^ low,) + span]
        if r == 0:
            return pltpu.make_async_copy(origin, down_b.at[(0,) + span], down_recv.at[0, j])
        return pltpu.make_async_remote_copy(
            src_ref=origin,
            dst_ref=down_b.at[(r,) + span],
            send_sem=down_send.at[r],
            recv_sem=down_recv.at[r, j],
            device_id={"tp": tp ^ low},
            device_id_type=MESH,
        )

    def row_copy(r, u, i):
        low = r & -r
        return pltpu.make_async_remote_copy(
            src_ref=arrived.at[u, i, r ^ low],
            dst_ref=arrived.at[u, i, r],
            send_sem=row_send.at[r],
            recv_sem=row_recv.at[relays.index(r), u, i] if r in relays else leaf_recv.at[r, u],
            device_id={"tp": tp ^ low},
            device_id_type=MESH,
        )

    def everything(ref, send, recv):
        return pltpu.make_async_remote_copy(
            src_ref=ref,
            dst_ref=ref,
            send_sem=send,
            recv_sem=recv,
            device_id={"ep": peer(1)},
            device_id_type=MESH,
        )

    def start_down(first, last):
        @pl.loop(first, last)
        def _(j):
            for r in forwards[0]:
                down_copy(r, j).start()

    @pl.loop(0, D_CHUNKS)
    def _(j):
        down_copy(0, j).start()

    pl.semaphore_wait(barrier, n_ep - 1 + n_tp - 1)
    start_down(0, FIRST)

    for load in loads[:4]:
        load.wait()
    mine = pl.ds(aligned(tp, tokens), tokens)
    own = named[:, mine]
    own_share = shares[:, mine]
    top = own.shape[0]
    experts = lax.broadcasted_iota(jnp.int32, (n_ep, tokens), 0)
    onehot = [
        (experts == jnp.broadcast_to(own[k : k + 1, :], (n_ep, tokens))).astype(jnp.float32)
        for k in range(top)
    ]
    per_token = functools.reduce(lambda a, b: a + b, onehot)
    before = (
        lax.broadcasted_iota(jnp.int32, (tokens, tokens), 0)
        < lax.broadcasted_iota(jnp.int32, (tokens, tokens), 1)
    ).astype(jnp.bfloat16)
    earlier = jnp.dot(per_token.astype(jnp.bfloat16), before, preferred_element_type=jnp.float32)
    slot_rows = lax.broadcasted_iota(jnp.int32, (slots, tokens), 0)
    picked = jnp.zeros((slots, tokens), jnp.float32)
    spread = jnp.zeros((slots, tokens), jnp.float32)
    shift = sub.bit_length() - 1
    for k in range(top):
        rank = jnp.sum(onehot[k] * earlier, axis=0, keepdims=True).astype(jnp.int32)
        away = jnp.bitwise_xor(own[k : k + 1, :], ep)
        turn = lax.shift_right_logical(rank, jnp.full_like(rank, shift))
        far = jnp.where(away >= group, 1, 0)
        slot = ((far * rounds + turn) * group + away - far * group) * sub + rank - turn * sub
        match = slot_rows == jnp.broadcast_to(slot, (slots, tokens))
        picked = picked + jnp.where(match, 1.0, 0.0)
        spread = spread + jnp.where(
            match, jnp.broadcast_to(own_share[k : k + 1, :], (slots, tokens)), 0.0
        )
    picked = picked.reshape(2, rounds, group * sub, tokens).astype(jnp.bfloat16)
    for half in range(2):
        pick[:, half * group * sub : (half + 1) * group * sub, :] = picked[half]
    spread = spread.T
    high = spread.astype(jnp.bfloat16)
    low = (spread - high.astype(jnp.float32)).astype(jnp.bfloat16)
    for i, part in enumerate((high, low)):
        share_near[i] = part[:, : slots // 2]
        share_far[i] = part[:, slots // 2 :]
    share_copy = pltpu.make_async_remote_copy(
        src_ref=share_far,
        dst_ref=share_in.at[1 - inner],
        send_sem=share_send,
        recv_sem=share_recv.at[1 - inner],
        device_id={"ep": peer(group + quarter * inner)},
        device_id_type=MESH,
    )

    @pl.loop(0, tokens // NORM_ROWS)
    def _(i):
        at = aligned(i, NORM_ROWS)
        normed[pl.ds(at, NORM_ROWS), :] = norm_rows(x_in, e_gain, at)

    def send_rows(u, i):
        half = u // rounds
        return pltpu.make_async_remote_copy(
            src_ref=outgoing.at[u, i],
            dst_ref=arrived.at[u, i, 0],
            send_sem=out_send.at[half, i],
            recv_sem=out_recv.at[u, i],
            device_id={"ep": peer(half * group + i)},
            device_id_type=MESH,
        )

    sequence = [0, rounds] + list(range(1, rounds)) + list(range(rounds + 1, n_groups))

    def send_group(u):
        @pl.loop(0 if u >= rounds else 1, group)
        def _(i):
            send_rows(u, i).start()

    for k in range(rounds):
        rows = jnp.dot(pick[k], normed[...], preferred_element_type=jnp.float32)
        rows = rows.astype(jnp.bfloat16).reshape(2, group, sub, width)
        arrived[k, 0, 0] = rows[0, 0]
        for half in range(2):
            outgoing[half * rounds + k] = rows[half]
        for r in forwards[0]:
            row_copy(r, k, 0).start()
        for u in (0, rounds) if k == 0 else (k,):
            send_group(u)
    for u in range(rounds + 1, n_groups):
        send_group(u)

    for load in loads[4:]:
        load.wait()

    @pl.loop(0, tokens // NORM_ROWS)
    def _(i):
        at = aligned(i, NORM_ROWS)
        rows = norm_rows(m_in, m_gain, at)
        for g in range(n_tp):
            m_normed[g, pl.ds(at, NORM_ROWS), :] = rows[:, g * group_width : (g + 1) * group_width]

    own_rows = pl.ds(pl.multiple_of(WMAX + tp * tokens, WMAX), tokens)
    m_rows[own_rows, :] = m_normed[tp]

    last = n_tp - 1

    def tail_copy(r):
        return pltpu.make_async_remote_copy(
            src_ref=m_normed.at[last ^ r, tokens - WMAX : tokens, :],
            dst_ref=m_tail,
            send_sem=tail_send.at[r],
            recv_sem=tail_recv,
            device_id={"tp": tp ^ r},
            device_id_type=MESH,
        )

    halo = pltpu.make_async_remote_copy(
        src_ref=m_tail,
        dst_ref=m_rows.at[0:WMAX, :],
        send_sem=halo_send,
        recv_sem=halo_recv,
        device_id={"ep": lax.rem(ep + 1, n_ep)},
        device_id_type=MESH,
    )

    @pl.when(tp == last)
    def _():
        for r in range(1, n_tp):
            tail_copy(r).start()
        m_tail[...] = m_normed[last, tokens - WMAX : tokens, :]


    def send_mix(r):
        return pltpu.make_async_remote_copy(
            src_ref=m_normed.at[tp ^ r],
            dst_ref=m_rows.at[own_rows, :],
            send_sem=mix_send.at[r],
            recv_sem=mix_recv.at[r],
            device_id={"tp": tp ^ r},
            device_id_type=MESH,
        )

    def take(u):
        @pl.loop(0 if u >= rounds else 1, group)
        def _(i):
            send_rows(u, i).wait_recv()
            for r in forwards[0]:
                row_copy(r, u, i).start()

    def relay(u):
        for r in relays:

            @pl.loop(0, group)
            def _(i):
                row_copy(r, u, i).wait_recv()
                for target in forwards[r]:
                    row_copy(target, u, i).start()

    def hid_copy(r, u):
        return pltpu.make_async_remote_copy(
            src_ref=hidden_out.at[u, r],
            dst_ref=hidden.at[u, :, :, r * part_units : (r + 1) * part_units],
            send_sem=hid_send.at[r],
            recv_sem=hid_recv.at[r],
            device_id={"tp": tp ^ r},
            device_id_type=MESH,
        )

    def work(u):
        for r in leaves:
            everything(arrived.at[u, :, r], row_send.at[r], leaf_recv.at[r, u]).wait_recv()

        @pl.loop(0, K_CHUNKS)
        def _(k):
            span = pl.ds(aligned(k, k_size), k_size)
            rows = arrived[u, :, :, :, span].reshape(group * n_tp * sub, k_size)
            product = jnp.dot(rows, gate_up[span, :], preferred_element_type=jnp.float32)

            @pl.when(k == 0)
            def _():
                acc[...] = product

            @pl.when(k > 0)
            def _():
                acc[...] += product

        units_of = clamped_unit(acc[:, :part_units], acc[:, part_units:])
        units_of = units_of.reshape(group, n_tp, sub, part_units)
        hidden[u, :, :, 0:part_units] = units_of[:, 0]
        for r in range(1, n_tp):
            hidden_out[u, r] = units_of[:, r]
            hid_copy(r, u).start()

    for step in range(len(sequence) + 2):
        if step < len(sequence):
            take(sequence[step])
        if step == min(1, len(sequence) - 1):

            @pl.when(tp != last)
            def _():
                tail_copy(1).wait_recv()

            halo.start()
        if step == len(sequence):
            share_copy.start()
        if step == len(sequence) and step >= 2:
            work(sequence[step - 2])
            start_down(FIRST, SECOND)
        if 1 <= step <= len(sequence):
            relay(sequence[step - 1])
        if step >= 2 and step != len(sequence) or step == len(sequence) + 1:
            work(sequence[step - 2])

    start_down(SECOND, D_CHUNKS)
    for r in range(1, n_tp):
        send_mix(r).start()

    for r in range(1, n_tp):
        mine = hidden.at[:, :, :, r * part_units : (r + 1) * part_units]
        everything(mine, hid_send.at[r], hid_recv.at[r]).wait_recv()

    far = slice(rounds, n_groups)

    def send_back(j, i):
        return pltpu.make_async_remote_copy(
            src_ref=result.at[j, 0:rounds, i],
            dst_ref=returned.at[j, :, i],
            send_sem=ret_send.at[i],
            recv_sem=ret_recv.at[j],
            device_id={"ep": peer(i)},
            device_id_type=MESH,
        )

    def send_near(j):
        @pl.loop(1, group)
        def _(i):
            send_back(j, i).start()

    def bit_of(i):
        return lax.rem(lax.div(i, quarter), 2)

    def collect(j, i, kind, step):
        return pltpu.make_async_remote_copy(
            src_ref=result.at[j, far, i],
            dst_ref=gathered.at[kind, j, :, i],
            send_sem=col_send.at[i],
            recv_sem=col_recv.at[kind, j],
            device_id={"ep": peer(step)},
            device_id_type=MESH,
        )

    def collect_out(j, i):
        kind = jnp.bitwise_xor(bit_of(i), inner)
        step = lax.rem(i, quarter) + (1 - inner) * quarter
        return kind, step

    def partial_copy(kind, j):
        return pltpu.make_async_remote_copy(
            src_ref=partial_out.at[kind, j],
            dst_ref=partial_in.at[j],
            send_sem=part_send.at[kind],
            recv_sem=part_recv.at[j],
            device_id={"ep": peer(group + (1 - kind) * quarter)},
            device_id_type=MESH,
        )

    def sum_far(j):
        @pl.when(inner == 1)
        def _():
            for kind in (1, 0):

                several = gathered.at[kind, j, :, 0 : group - 1]
                everything(several, col_send.at[0], col_recv.at[kind, j]).wait_recv()
                rows = gathered[kind, j].reshape(slots // 2, d_size)
                partial_out[kind, j] = (
                    jnp.dot(share_in[kind, 0], rows, preferred_element_type=jnp.float32)
                    + jnp.dot(share_in[kind, 1], rows, preferred_element_type=jnp.float32)
                ).astype(jnp.bfloat16)
                partial_copy(kind, j).start()

    def down_arrive(j):
        down_copy(0, j).wait()
        for r in relays:
            down_copy(r, j).wait_recv()
            for target in forwards[r]:
                down_copy(target, j).start()
        for r in leaves:
            down_copy(r, j).wait_recv()

    @pl.when(inner == 1)
    def _():
        for kind in range(2):
            pltpu.make_async_remote_copy(
                src_ref=share_far,
                dst_ref=share_in.at[kind],
                send_sem=share_send,
                recv_sem=share_recv.at[kind],
                device_id={"ep": peer(group)},
                device_id_type=MESH,
            ).wait_recv()

    @pl.loop(0, D_CHUNKS)
    def _(j):
        down_arrive(j)
        weight = down_b[:, :, pl.ds(aligned(j, d_size), d_size)].reshape(units, d_size)
        rows = hidden[...].reshape(slots, units)
        product = jnp.dot(rows, weight, preferred_element_type=jnp.float32)
        result[j] = product.astype(jnp.bfloat16).reshape(n_groups, group, sub, d_size)

        @pl.loop(0, group)
        def _(i):
            kind, step = collect_out(j, i)

            @pl.when(step > 0)
            def _():
                collect(j, i, kind, step).start()

            @pl.when(step == 0)
            def _():
                gathered[kind, j, :, i] = result[j, far, i]

        returned[j, :, 0] = result[j, 0:rounds, 0]

        @pl.when(j >= near_lag)
        def _():
            send_near(j - near_lag)

        @pl.when(j >= lag)
        def _():
            sum_far(j - lag)

    @pl.loop(D_CHUNKS - near_lag, D_CHUNKS)
    def _(j):
        send_near(j)

    @pl.loop(D_CHUNKS - lag, D_CHUNKS)
    def _(j):
        sum_far(j)

    for r in range(1, n_tp):
        theirs = pl.ds(pl.multiple_of(WMAX + (tp ^ r) * tokens, WMAX), tokens)
        pltpu.make_async_remote_copy(
            src_ref=m_normed.at[tp ^ r],
            dst_ref=m_rows.at[theirs, :],
            send_sem=mix_send.at[r],
            recv_sem=mix_recv.at[r],
            device_id={"tp": tp ^ r},
            device_id_type=MESH,
        ).wait_recv()
    halo.wait_recv()
    window = 2 << tp
    span_rows = tokens + WMAX
    here = lax.broadcasted_iota(jnp.int32, (tokens, span_rows), 0)
    there = lax.broadcasted_iota(jnp.int32, (tokens, span_rows), 1)
    back = here + WMAX - there
    inside = (back >= 0) & (back < window)
    row = lax.broadcasted_iota(jnp.int32, (tokens, 1), 0)
    stores = []
    for b in range(n_tp):
        position = (ep * n_tp + b) * tokens
        band = (inside & (there + position >= WMAX)).astype(jnp.bfloat16)
        values = m_rows[b * tokens : b * tokens + span_rows, :]
        total = jnp.dot(band, values, preferred_element_type=jnp.float32)
        counts = jnp.minimum(row + position + 1, window).astype(jnp.float32)
        pooled = (total / counts - values[WMAX:, :].astype(jnp.float32)).astype(jnp.bfloat16)
        product = jnp.dot(pooled, g_weight[...], preferred_element_type=jnp.float32)
        m_out[b] = (product * scale[...]).astype(jnp.bfloat16)
        store = pltpu.make_async_copy(
            m_out.at[b], mixed_out.at[b * tokens : (b + 1) * tokens, :], m_store.at[b]
        )
        store.start()
        stores.append(store)

    def write_out(j):
        return pltpu.make_async_copy(
            e_out.at[j], expert_out.at[:, pl.ds(aligned(j, d_size), d_size)], e_store
        )

    @pl.loop(0, D_CHUNKS)
    def _(j):
        everything(returned.at[j, :, 1:group], ret_send.at[0], ret_recv.at[j]).wait_recv()
        partial_copy(0, j).wait_recv()
        rows = returned[j].reshape(slots // 2, d_size)
        e_out[j] = (
            jnp.dot(share_near[0], rows, preferred_element_type=jnp.float32)
            + jnp.dot(share_near[1], rows, preferred_element_type=jnp.float32)
            + partial_in[j].astype(jnp.float32)
        ).astype(jnp.bfloat16)
        write_out(j).start()

    for r in range(1, n_tp):
        everything(down_b.at[r], down_send.at[r], down_recv.at[r, 0]).wait_send()
        everything(hidden_out.at[:, r], hid_send.at[r], hid_recv.at[r]).wait_send()
        everything(arrived.at[:, :, r], row_send.at[r], hid_recv.at[r]).wait_send()
        send_mix(r).wait_send()
    halo.wait_send()
    share_copy.wait_send()

    @pl.when(tp == last)
    def _():
        for r in range(1, n_tp):
            tail_copy(r).wait_send()

    for half in range(2):
        rows_of = slice(half * rounds, (half + 1) * rounds)

        @pl.loop(1 - half, group)
        def _(i):
            everything(outgoing.at[rows_of, i], out_send.at[half, i], share_send).wait_send()

    @pl.loop(1, group)
    def _(i):
        everything(result.at[:, 0:rounds, i], ret_send.at[i], share_send).wait_send()

    @pl.loop(0, group)
    def _(i):
        _, step = collect_out(0, i)

        @pl.when(step > 0)
        def _():
            everything(result.at[:, far, i], col_send.at[i], share_send).wait_send()

    @pl.when(inner == 1)
    def _():
        for kind in range(2):
            everything(partial_out.at[kind], part_send.at[kind], share_send).wait_send()

    everything(e_out, share_send, e_store).wait_recv()
    for store in stores:
        store.wait()


def shards(
    mixer_in,
    mixer_gain,
    group_weight,
    group_scale,
    expert_in,
    expert_gain,
    routes,
    route_weight,
    gate_weight,
    up_weight,
    down_weight,
):
    n_ep = lax.axis_size("ep")
    n_tp = lax.axis_size("tp")
    tokens, width = expert_in.shape
    group_width = group_weight.shape[-1]
    block_tokens, top = routes.shape
    part_units = gate_weight.shape[-1]
    units = part_units * n_tp
    capacity = max(2, 3 * tokens * top // (2 * n_ep))
    capacity = -(-capacity // 8) * 8
    slots = n_ep * capacity
    sub = 16 if capacity % 16 == 0 else 8
    rounds = capacity // sub
    groups = 2 * rounds
    group = n_ep // 2
    d_size = width // D_CHUNKS
    bf16, f32 = jnp.bfloat16, jnp.float32
    vmem = pltpu.VMEM
    dma = pltpu.SemaphoreType.DMA
    anywhere = pl.BlockSpec(memory_space=pl.ANY)
    scratch = [
        vmem((tokens, width), bf16),
        vmem((tokens, width), bf16),
        vmem((1, width), f32),
        vmem((1, width), f32),
        vmem((1, group_width), f32),
        vmem((top, block_tokens), jnp.int32),
        vmem((top, block_tokens), f32),
        vmem((width, 2 * part_units), bf16),
        vmem((n_tp, part_units, width), bf16),
        vmem((tokens, width), bf16),
        vmem((rounds, n_ep * sub, tokens), bf16),
        vmem((2, tokens, slots // 2), bf16),
        vmem((2, tokens, slots // 2), bf16),
        vmem((2, 2, tokens, slots // 2), bf16),
        vmem((groups, group, sub, width), bf16),
        vmem((groups, group, n_tp, sub, width), bf16),
        vmem((group * n_tp * sub, 2 * part_units), f32),
        vmem((groups, n_tp, group, sub, part_units), bf16),
        vmem((groups, group, sub, units), bf16),
        vmem((D_CHUNKS, groups, group, sub, d_size), bf16),
        vmem((D_CHUNKS, rounds, group, sub, d_size), bf16),
        vmem((2, D_CHUNKS, rounds, group, sub, d_size), bf16),
        vmem((2, D_CHUNKS, tokens, d_size), bf16),
        vmem((D_CHUNKS, tokens, d_size), bf16),
        vmem((n_tp, tokens, group_width), bf16),
        vmem((WMAX + n_tp * tokens, group_width), bf16),
        vmem((WMAX, group_width), bf16),
        vmem((group_width, group_width), bf16),
        vmem((n_tp, tokens, group_width), bf16),
        vmem((D_CHUNKS, tokens, d_size), bf16),
        dma((10,)),
        dma((n_tp,)),
        dma((n_tp, D_CHUNKS)),
        dma((2, group)),
        dma((groups, group)),
        dma((n_tp,)),
        dma((max(1, n_tp // 2 - 1), groups, group)),
        dma((n_tp, groups)),
        dma((n_tp,)),
        dma((n_tp,)),
        dma((group,)),
        dma((D_CHUNKS,)),
        dma(()),
        dma((2,)),
        dma((group,)),
        dma((2, D_CHUNKS)),
        dma((2,)),
        dma((D_CHUNKS,)),
        dma((n_tp,)),
        dma((n_tp,)),
        dma((n_tp,)),
        dma(()),
        dma(()),
        dma(()),
        dma((n_tp,)),
        dma(()),
    ]
    flops = 6 * slots * width * units + 2 * n_tp * tokens * group_width * group_width
    return pl.pallas_call(
        functools.partial(kernel, n_ep, n_tp),
        out_shape=(
            jax.ShapeDtypeStruct((n_tp * tokens, group_width), bf16),
            jax.ShapeDtypeStruct((tokens, width), bf16),
        ),
        in_specs=[anywhere] * 11,
        out_specs=(anywhere, anywhere),
        scratch_shapes=scratch,
        compiler_params=pltpu.CompilerParams(
            collective_id=0, has_side_effects=True, vmem_limit_bytes=67043328
        ),
        cost_estimate=pl.CostEstimate(flops=flops, bytes_accessed=1 << 26, transcendentals=0),
    )(
        mixer_in,
        mixer_gain.reshape(1, width),
        group_weight,
        group_scale,
        expert_in,
        expert_gain.reshape(1, width),
        routes.T,
        route_weight.T,
        gate_weight,
        up_weight,
        down_weight,
    )


def solution(mesh):
    in_specs = (
        P(("ep", "tp"), None),
        P(),
        P("tp", None, None),
        P("tp", None),
        P(("ep", "tp"), None),
        P(),
        P("ep", None),
        P("ep", None),
        P("ep", None, "tp"),
        P("ep", None, "tp"),
        P("ep", "tp", None),
    )
    out_specs = (P("ep", "tp"), P(("ep", "tp"), None))
    return jax.shard_map(shards, mesh=mesh, in_specs=in_specs, out_specs=out_specs, check_vma=False)
```
